32 devices in a mesh: ep: 8 (over z, x), tp: 4 (over y, core).
Axes of the slice: x: 2, y: 2, z: 4, core: 2. Of those that a mesh axis runs over, the one named last changes fastest.
Arguments:
- conv_input: bfloat16 [4096, 2048], P(('ep', 'tp')), may hold values from -6 to 6
- conv_kernel: float32 [31, 2048], replicated, may hold values from -1 to 1
- conv_gain: float32 [2048], replicated, may hold values from 0.1 to 1.9
- out_weight: bfloat16 [2048, 2048], P(None, 'tp'), may hold values from -0.125 to 0.125
- moe_input: bfloat16 [4096, 2048], P(('ep', 'tp')), may hold values from -6 to 6
- moe_gain: float32 [2048], replicated, may hold values from 0.1 to 1.9
- expert_gate: bfloat16 [8, 2048, 2048], P('ep', None, 'tp'), may hold values from -0.125 to 0.125
- expert_up: bfloat16 [8, 2048, 2048], P('ep', None, 'tp'), may hold values from -0.125 to 0.125
- expert_down: bfloat16 [8, 2048, 2048], P('ep', 'tp'), may hold values from -0.125 to 0.125
- shared_gate: bfloat16 [2048, 128], replicated, may hold values from -0.125 to 0.125
- shared_up: bfloat16 [2048, 128], replicated, may hold values from -0.125 to 0.125
- shared_down: bfloat16 [128, 2048], replicated, may hold values from -0.5 to 0.5
- expert_index: int32 [4096, 2], P('ep'), may hold values from 0 to 7, all different within a row; in each aligned block of 128 rows (0 to 127, 128 to 255, ...) at most 48 rows name the same one
- routing_weight: float32 [4096, 2], P(('ep', 'tp')), may hold values from 0.25 to 1.5
Outputs:
- conv_out: bfloat16 [4096, 2048], P('ep', 'tp')
- moe_out: bfloat16 [4096, 2048], P(('ep', 'tp'))
The draws below stay inside these ranges and needn't reach their ends.
Inputs may be any that keep to these rules, and one draw needn't show every extreme that they name: `expert_index`: each row names 2 different experts. In each aligned block of 128 rows no expert is named by more than 48 of the rows, and in some blocks one expert is named by exactly 48 rows.
All inputs are finite; a program needn't handle non-finite values.
Results may differ from the reference program's by a relative error of at most 0.009.
Values may be sent and summed in bfloat16 or wider, within the bound.
A program may use at most 128 MiB of HBM per device.

```python
import math
import jax
import jax.numpy as jnp
import numpy as np
from jax import lax

D = 2048
FF = 2048
SHARED_FF = 128
TOPK = 2
KERNEL = 31
TOK_DEV_B = 128
TOKENS_A = 4096
TOKENS_B = 4096
EXPERTS = 8
SLOTS = 48
N_TP = 4


def level_of(key, dims, cuts, smallest, largest):
    def one(axis_at, blocks):
        heights = jax.random.uniform(jax.random.fold_in(jax.random.fold_in(key, 6), axis_at), (blocks,), jnp.float32, smallest / len(cuts), largest / len(cuts))
        return jnp.repeat(jnp.exp(heights), dims[axis_at] // blocks).reshape((-1,) + (1,) * (len(dims) - axis_at - 1))

    level = one(*cuts[0])
    for cut in cuts[1:]:
        level = level * one(*cut)
    return level


def shared_out(key, own, number, rows, number_of, top, limit, slope):
    sequence = jax.random.permutation(key, number_of)
    crowded, common = shares(number_of, rows * top, limit, slope, True), shares(number_of, rows * top, limit, slope, False)
    places = jnp.arange(number_of)

    def named(sizes, rotation):
        used = int((sizes > 0).sum())
        fixed = max(1, used // 4)
        moved = fixed + (places - fixed + rotation * (used - fixed)) % max(1, number_of - fixed)
        return jnp.zeros((number_of,), jnp.int32).at[sequence[jnp.where(places < fixed, places, moved)]].set(jnp.asarray(sizes, jnp.int32))

    sizes = jnp.where(number % 4 == 0, named(crowded, number // 4), named(common, number - number // 4 - 1))
    mixed = jax.random.permutation(jax.random.fold_in(own, 3), number_of)
    donor, receiver = mixed[0:number_of // 2 * 2:2], mixed[1:number_of // 2 * 2:2]
    slack = jnp.minimum(sizes[donor] - 1, limit - sizes[receiver]) // 2
    slack = jnp.where((donor == sequence[0]) | (receiver == sequence[0]) | (sizes[receiver] == 0), 0, jnp.maximum(slack, 0))
    moved = jax.random.randint(jax.random.fold_in(own, 4), (number_of // 2,), 0, 1 << 20) % (slack + 1)
    sizes = sizes.at[donor].add(-moved).at[receiver].add(moved)
    members = jnp.searchsorted(jnp.cumsum(sizes), jnp.arange(rows * top), side="right").astype(jnp.int32)
    grid = members.reshape(top, rows).T
    grid = grid[jax.random.permutation(jax.random.fold_in(own, 1), rows)]
    rotation = jax.random.randint(jax.random.fold_in(own, 2), (rows, 1), 0, top)
    return jnp.take_along_axis(grid, (jnp.arange(top)[None, :] + rotation) % top, axis=1)


def shares(count, total, bound, skew, full):
    weights = [(1 << 20) // math.isqrt(rank ** skew) + 1 for rank in range(1, count + 1)]
    largest = bound if full else min(bound, max(-(-total // count), total * weights[0] // sum(weights)))
    least = 1 if total - largest >= count - 1 else 0
    given, rest = [largest] + [least] * (count - 1), total - largest - least * (count - 1)
    while rest > 0:
        free = [i for i in range(1, count) if given[i] < largest] or [i for i in range(1, count) if given[i] < bound]
        pool, remaining = sum([weights[i] for i in free]), rest
        for i in free:
            addition = min(bound - given[i], max(1, remaining * weights[i] // pool), rest)
            given[i] = given[i] + addition
            rest = rest - addition
    return np.array(given)


def normal_values(key, extent, width, limit, split=(), kind=jnp.bfloat16):
    level = level_of(key, extent, split, -0.22, 0.18) if split else 1.0
    values = jax.random.normal(key, extent, jnp.float32) * width * level
    return jnp.minimum(jnp.maximum(values, -limit), limit).astype(kind)


def setup_inputs(seed: int = 0) -> dict:
    splits = jax.random.split(jax.random.key(seed), 15)
    conv_input = normal_values(splits[0], (TOKENS_A, D), 1.0, 6.0, ((0, 32),))
    conv_kernel = normal_values(splits[1], (KERNEL, D), KERNEL ** -0.5, 1.0, (), jnp.float32)
    conv_gain = jnp.clip(1.0 + 0.18 * jax.random.normal(splits[2], (D,), jnp.float32), 0.1, 1.9)
    out_weight = normal_values(splits[3], (D, D), D ** -0.5, 0.125, ((1, 4),))
    moe_input = normal_values(splits[4], (TOKENS_B, D), 1.0, 6.0, ((0, 32),))
    moe_gain = jnp.clip(1.0 + 0.18 * jax.random.normal(splits[5], (D,), jnp.float32), 0.1, 1.9)
    expert_gate = normal_values(splits[6], (EXPERTS, D, FF), D ** -0.5, 0.125, ((0, 8), (2, 4)))
    expert_up = normal_values(splits[7], (EXPERTS, D, FF), D ** -0.5, 0.125, ((0, 8), (2, 4)))
    expert_down = normal_values(splits[8], (EXPERTS, FF, D), FF ** -0.5, 0.125, ((0, 8), (1, 4)))
    shared_gate = normal_values(splits[9], (D, SHARED_FF), D ** -0.5, 0.125)
    shared_up = normal_values(splits[10], (D, SHARED_FF), D ** -0.5, 0.125)
    shared_down = normal_values(splits[11], (SHARED_FF, D), SHARED_FF ** -0.5, 0.5)
    expert_index_keys = jax.random.split(jax.random.fold_in(splits[12], 1), TOKENS_B // TOK_DEV_B)
    expert_index_turns = jax.random.permutation(jax.random.fold_in(splits[12], 3), TOKENS_B // TOK_DEV_B)
    expert_index = jax.vmap(lambda own, number: shared_out(jax.random.fold_in(splits[12], 2), own, number, TOK_DEV_B, EXPERTS, TOPK, SLOTS, 2))(expert_index_keys, expert_index_turns).reshape((TOKENS_B, TOPK))
    routing_weight = jnp.clip(0.25 + 1.25 * jax.random.uniform(splits[13], (TOKENS_B, TOPK), jnp.float32) ** level_of(splits[13], (TOKENS_B, TOPK), ((0, 32),), -0.2, 0.2), 0.25, 1.5)
    return dict(conv_input=conv_input, conv_kernel=conv_kernel, conv_gain=conv_gain, out_weight=out_weight, moe_input=moe_input, moe_gain=moe_gain, expert_gate=expert_gate, expert_up=expert_up, expert_down=expert_down, shared_gate=shared_gate, shared_up=shared_up, shared_down=shared_down, expert_index=expert_index, routing_weight=routing_weight)


NORM_EPS = 1e-05

def layer_scale(row_data, gain_vec):
    values = row_data.astype(jnp.float32)
    center = values - lax.optimization_barrier(jnp.mean(values, axis=-1, keepdims=True))
    spread = lax.optimization_barrier(jnp.mean(center * center, axis=-1, keepdims=True))
    return center * lax.rsqrt(spread + NORM_EPS) * gain_vec

def depthwise(padded, kernel, length):
    running = jnp.zeros((length, padded.shape[1]), jnp.float32)
    for offset in range(kernel.shape[0]):
        running = running + padded[offset:offset + length].astype(jnp.float32) * kernel[offset]
    return running

def slot_table(block_index, experts, slot_count):
    onehot = (block_index[:, :, None] == jnp.arange(experts, dtype=jnp.int32)[None, None, :]).astype(jnp.int32)
    before = jnp.cumsum(onehot, axis=1) - onehot
    position = lax.optimization_barrier(jnp.sum(before * onehot, axis=2))
    return (block_index * slot_count + position).astype(jnp.int32)

def reference(conv_input, conv_kernel, conv_gain, out_weight, moe_input, moe_gain, expert_gate, expert_up, expert_down, shared_gate, shared_up, shared_down, expert_index, routing_weight):
    length = conv_input.shape[0]
    padded = jnp.concatenate([jnp.zeros((KERNEL - 1, D), jnp.bfloat16), conv_input], axis=0)
    mixed_rows = depthwise(padded, conv_kernel, length)
    normed = jax.nn.silu(layer_scale(mixed_rows, conv_gain)).astype(jnp.bfloat16)
    conv_out = jnp.dot(normed, out_weight, preferred_element_type=jnp.float32).astype(jnp.bfloat16)
    normal = layer_scale(moe_input, moe_gain).astype(jnp.bfloat16)
    blocks = TOKENS_B // TOK_DEV_B
    entries = TOK_DEV_B * TOPK
    block_index = expert_index.reshape(blocks, entries)
    entry_slot = slot_table(block_index, EXPERTS, SLOTS)
    block_ids = jnp.arange(blocks, dtype=jnp.int32)[:, None]
    entry_row = block_ids * TOK_DEV_B + jnp.arange(entries, dtype=jnp.int32)[None, :] // TOPK
    slot_row = jnp.zeros((blocks, EXPERTS * SLOTS), jnp.int32).at[block_ids, entry_slot].set(entry_row)
    slot_weight = jnp.zeros((blocks, EXPERTS * SLOTS), jnp.float32).at[block_ids, entry_slot].set(routing_weight.reshape(blocks, entries))
    slot_row = slot_row.reshape(blocks, EXPERTS, SLOTS)
    slot_weight = slot_weight.reshape(blocks, EXPERTS, SLOTS)
    quarter = FF // N_TP

    def expert_step(running, expert_id):
        rows_of = lax.dynamic_index_in_dim(slot_row, expert_id, 1, keepdims=False).reshape(-1)
        weights = lax.dynamic_index_in_dim(slot_weight, expert_id, 1, keepdims=False).reshape(-1, 1)
        row_data = normal[rows_of]
        gate_proj = jnp.dot(row_data, expert_gate[expert_id], preferred_element_type=jnp.float32)
        up_proj = jnp.dot(row_data, expert_up[expert_id], preferred_element_type=jnp.float32)
        hidden = (jax.nn.silu(gate_proj) * up_proj).astype(jnp.bfloat16)
        down_all = expert_down[expert_id]
        summed = jnp.zeros((row_data.shape[0], D), jnp.float32)
        for index_q in range(N_TP):
            part_q = jnp.dot(hidden[:, index_q * quarter:(index_q + 1) * quarter], down_all[index_q * quarter:(index_q + 1) * quarter], preferred_element_type=jnp.float32).astype(jnp.bfloat16)
            summed = summed + lax.optimization_barrier(part_q).astype(jnp.float32)
        result = lax.optimization_barrier(summed.astype(jnp.bfloat16)).astype(jnp.float32)
        return (running.at[rows_of].add(weights * result), None)
    routed, _ = lax.scan(expert_step, jnp.zeros((TOKENS_B, D), jnp.float32), jnp.arange(EXPERTS, dtype=jnp.int32))
    shared_gate_proj = jnp.dot(normal, shared_gate, preferred_element_type=jnp.float32)
    shared_up_proj = jnp.dot(normal, shared_up, preferred_element_type=jnp.float32)
    shared_hidden = (jax.nn.silu(shared_gate_proj) * shared_up_proj).astype(jnp.bfloat16)
    shared_part = jnp.dot(shared_hidden, shared_down, preferred_element_type=jnp.float32)
    moe_out = (shared_part + routed).astype(jnp.bfloat16)
    return (conv_out, moe_out)
```

```python
import functools

import jax
import jax.numpy as jnp
from jax import lax
from jax.experimental import pallas as pl
from jax.experimental.pallas import tpu as pltpu
from jax.sharding import PartitionSpec as P

NORM_EPS = 1e-05


def passed_along(block, axis, distance):
    devices = range(lax.axis_size(axis))
    route = [(i - distance, i) for i in devices if i - distance in devices]
    return lax.ppermute(block, axis, route)


def layer_scale(row_data, gain_vec):
    values = row_data.astype(jnp.float32)
    center = values - jnp.mean(values, axis=-1, keepdims=True)
    spread = jnp.mean(center * center, axis=-1, keepdims=True)
    return center * lax.rsqrt(spread + NORM_EPS) * gain_vec


def depthwise(padded, kernel, length):
    running = jnp.zeros((length, padded.shape[1]), jnp.float32)
    for offset in range(kernel.shape[0]):
        running = running + padded[offset : offset + length].astype(jnp.float32) * kernel[offset]
    return running


def slot_table(block_index, experts, slot_count):
    onehot = (
        block_index[:, :, None] == jnp.arange(experts, dtype=jnp.int32)[None, None, :]
    ).astype(jnp.int32)
    before = jnp.cumsum(onehot, axis=1) - onehot
    position = jnp.sum(before * onehot, axis=2)
    return block_index * slot_count + position


def fill_slots(row_data, entry_slot, top_count, total_slots):
    block_count = entry_slot.shape[0]
    entries = entry_slot.shape[1]
    block_ids = jnp.arange(block_count, dtype=jnp.int32)[:, None]
    source = jnp.arange(entries, dtype=jnp.int32)[None, :] // top_count
    slot_row = (
        jnp.zeros((block_count, total_slots), jnp.int32).at[block_ids, entry_slot].set(source)
    )
    filled = jnp.zeros((block_count, total_slots), jnp.int32).at[block_ids, entry_slot].set(1)
    picked = row_data[block_ids, slot_row]
    return jnp.where(filled[:, :, None] > 0, picked, jnp.zeros((), row_data.dtype))


def gated(row_data, gate_weight, up_weight):
    gate_proj = jnp.dot(row_data, gate_weight, preferred_element_type=jnp.float32)
    up_proj = jnp.dot(row_data, up_weight, preferred_element_type=jnp.float32)
    return (jax.nn.silu(gate_proj) * up_proj).astype(jnp.bfloat16)


def on_device(
    conv_input,
    conv_kernel,
    conv_gain,
    out_weight,
    moe_input,
    moe_gain,
    expert_gate,
    expert_up,
    expert_down,
    shared_gate,
    shared_up,
    shared_down,
    expert_index,
    routing_weight,
):
    reach = conv_kernel.shape[0] - 1
    length = conv_input.shape[0]
    halo_rows = passed_along(conv_input[length - reach :], ("ep", "tp"), 1)
    padded = jnp.concatenate([halo_rows, conv_input], axis=0)
    mixed_rows = depthwise(padded, conv_kernel, length)
    normed = jax.nn.silu(layer_scale(mixed_rows, conv_gain)).astype(jnp.bfloat16)
    conv_out = jnp.dot(
        lax.all_gather(normed, "tp", axis=0, tiled=True),
        out_weight,
        preferred_element_type=jnp.float32,
    ).astype(jnp.bfloat16)
    tp_parts = lax.axis_size("tp")
    tp_index = lax.axis_index("tp")
    ep_ranks = lax.axis_size("ep")
    tok_count = moe_input.shape[0]
    top_count = routing_weight.shape[1]
    model_width = moe_input.shape[1]
    experts = ep_ranks * expert_gate.shape[0]
    slot_count = 3 * tok_count * top_count // (2 * experts)
    total_slots = experts * slot_count
    normal = layer_scale(moe_input, moe_gain).astype(jnp.bfloat16)
    group_slots = slot_table(
        expert_index.reshape(tp_parts, tok_count * top_count), experts, slot_count
    )
    own_slots = lax.dynamic_index_in_dim(group_slots, tp_index, 0, keepdims=True)
    gate_local = expert_gate[0]
    up_local = expert_up[0]
    down_local = expert_down[0]
    own_rows = fill_slots(normal[None], own_slots, top_count, total_slots)
    own_rows = own_rows.reshape(ep_ranks, slot_count, model_width)
    arrived = lax.all_to_all(own_rows, "ep", split_axis=0, concat_axis=0, tiled=True)
    hidden = gated(
        lax.all_gather(
            arrived.reshape(ep_ranks * slot_count, model_width), "tp", axis=0, tiled=True
        ),
        gate_local,
        up_local,
    )
    summed = lax.psum_scatter(
        jnp.dot(hidden, down_local, preferred_element_type=jnp.float32).astype(jnp.bfloat16),
        "tp",
        scatter_dimension=0,
        tiled=True,
    )
    returned = lax.all_to_all(
        summed.reshape(ep_ranks, slot_count, model_width),
        "ep",
        split_axis=0,
        concat_axis=0,
        tiled=True,
    )
    picked = returned.reshape(total_slots, model_width)[own_slots[0]]
    picked = picked.reshape(tok_count, top_count, model_width).astype(jnp.float32)
    routed = jnp.sum(picked * routing_weight[:, :, None], axis=1)
    shared_hidden = gated(normal, shared_gate, shared_up)
    shared_part = jnp.dot(shared_hidden, shared_down, preferred_element_type=jnp.float32)
    moe_out = (shared_part + routed).astype(jnp.bfloat16)
    return (conv_out, moe_out)


LANES = 128
ROW_TILE = 16
COLS = 512
CONV_PARTS = 4
MESH = pl.DeviceIdType.MESH


def fused_kernel(
    n,
    slots,
    reach,
    conv_hbm,
    taps_hbm,
    conv_gain,
    out_w_hbm,
    moe_hbm,
    moe_gain,
    gate_hbm,
    up_hbm,
    down_hbm,
    sh_gate_hbm,
    sh_up_hbm,
    sh_down_hbm,
    index_ref,
    weight_ref,
    conv_out,
    moe_out,
    own,
    own_peer,
    gath,
    part,
    from_core,
    pair_sum,
    from_y,
    result,
    result_peer,
    returned,
    returned_peer,
    normal,
    normal_peer,
    weight_peer,
    near_send,
    near_recv,
    total,
    halo,
    pad,
    mixed,
    conv_all,
    conv_in,
    taps,
    moe_in,
    gate_w,
    up_w,
    down_w,
    sh_gate,
    sh_up,
    sh_down,
    out_w,
    local_sem,
    chunk_send,
    chunk_recv,
    conv_send,
    conv_recv,
):
    tokens, width = moe_hbm.shape
    e = lax.axis_index("ep")
    t = lax.axis_index("tp")
    core = lax.rem(t, 2)
    row = t // 2
    core_peer = row * 2 + (1 - core)
    y_peer = (1 - row) * 2 + core
    diagonal = (1 - row) * 2 + (1 - core)
    place = e * 4 + t
    after = lax.rem(place + 1, n * 4)
    ahead = lax.rem(place + n * 4 - 1, n * 4)
    halo_rows = halo.shape[0]
    half = n // 2
    side = e // half
    deep = lax.rem(e, half) // 2
    across = lax.rem(e, 2)
    outer = side * deep + (1 - side) * (1 - deep)
    conv_cut = tokens // CONV_PARTS

    fetches = [
        pltpu.make_async_copy(src, dst, local_sem.at[i])
        for i, (src, dst) in enumerate(
            (
                (moe_hbm, moe_in),
                (conv_hbm, conv_in),
                (taps_hbm, taps),
                (gate_hbm.at[0], gate_w),
                (up_hbm.at[0], up_w),
                (down_hbm.at[0], down_w),
                (sh_gate_hbm, sh_gate),
                (sh_up_hbm, sh_up),
                (sh_down_hbm, sh_down),
                (out_w_hbm, out_w),
            )
        )
    ]
    for fetch in fetches:
        fetch.start()

    barrier = pltpu.get_barrier_semaphore()
    greeted = [(lax.rem(e + k, n), t) for k in range(1, n)]
    greeted += [(e, core_peer), (e, y_peer)]
    greeted += [(after // 4, lax.rem(after, 4)), (ahead // 4, lax.rem(ahead, 4))]
    for device in greeted:
        pl.semaphore_signal(barrier, inc=1, device_id=device, device_id_type=MESH)

    def flip(a, b):
        return a + b - 2 * a * b

    def near_rank(j):
        return side * half + 2 * flip(deep, j // 2) + flip(across, lax.rem(j, 2))

    def far_rank(there, j):
        return (1 - side) * half + 2 * there + flip(across, j)

    def near_item(j):
        return 0 if j == 0 else j + 1

    def is_far(k):
        return (k == 1) | (k > half)

    def far_parts(k):
        v = (k // (half + 1)) * (k - half)
        return v // 2, lax.rem(v, 2)

    def remote(src, dst, kind, k, device, k_there=None):
        return pltpu.make_async_remote_copy(
            src_ref=src,
            dst_ref=dst,
            send_sem=chunk_send.at[kind, k],
            recv_sem=chunk_recv.at[kind, k if k_there is None else k_there],
            device_id=device,
            device_id_type=MESH,
        )

    def conv_copy(src, dst, kind, device):
        return pltpu.make_async_remote_copy(
            src_ref=src,
            dst_ref=dst,
            send_sem=conv_send.at[kind],
            recv_sem=conv_recv.at[kind],
            device_id=device,
            device_id_type=MESH,
        )

    def send_near(j):
        k = near_item(j)
        return remote(own.at[j], gath.at[k, t], 0, j, (near_rank(j), t), k)

    def send_near_peer(j):
        k = near_item(j)
        return remote(own_peer.at[j], gath.at[k, y_peer], 1, k, (near_rank(j), t))

    def send_far(there, j):
        k = (1 + (half + 1) * outer) if j == 0 else (half + 1 + 2 * outer)
        s = half + 2 * there + j
        return remote(own.at[s], gath.at[k, t], 0, s, (far_rank(there, j), t), k)

    def arrive(k):
        return remote(own.at[k], gath.at[k, t], 0, k, (e, core_peer))

    def share_core(k, q):
        return remote(gath.at[k, q], gath.at[k, q], 2, k, (e, core_peer))

    def share_y(k, q):
        return remote(gath.at[k, q], gath.at[k, q], 1, k, (e, y_peer))

    def forward_core(k, q):
        return remote(gath.at[k, q], gath.at[k, q], 3, k, (e, core_peer))

    def reduce_core(k, q, which):
        return remote(part.at[k, q], from_core.at[which, k], 4 + which, k, (e, core_peer))

    def reduce_y(k):
        return remote(pair_sum.at[k], from_y.at[k], 6, k, (e, y_peer))

    def return_near(k):
        j = k - 1
        return remote(result.at[k], returned.at[j], 7, k, (near_rank(j), t), j)

    def return_near_peer(k):
        j = k - 1
        return remote(result_peer.at[k], returned_peer.at[j], 8, k, (near_rank(j), t), j)

    def return_far(k):
        m, j = far_parts(k)
        there = m * (1 - side) + (1 - m) * side
        s = half + 2 * deep + j
        return remote(result.at[k], returned.at[s], 7, k, (far_rank(there, j), t), s)

    normal_y = conv_copy(normal, normal_peer, 1, (e, y_peer))
    weight_y = conv_copy(weight_ref, weight_peer, 2, (e, y_peer))
    halo_copy = conv_copy(
        conv_in.at[pl.ds(tokens - halo_rows, halo_rows)],
        halo,
        0,
        (after // 4, lax.rem(after, 4)),
    )
    conv_core = conv_copy(conv_all.at[t], conv_all.at[t], 3, (e, core_peer))
    conv_pass = conv_copy(conv_all.at[y_peer], conv_all.at[y_peer], 4, (e, core_peer))
    near_y = conv_copy(near_send, near_recv, 5, (e, y_peer))

    def conv_y(q, p):
        block = conv_all.at[q, pl.ds(p * conv_cut, conv_cut)]
        return conv_copy(block, block, 6 + p, (e, y_peer))

    fetches[0].wait()

    def normal_rows(i, carry):
        rows = pl.ds(pl.multiple_of(i * ROW_TILE, ROW_TILE), ROW_TILE)
        normal[rows, :] = layer_scale(moe_in[rows, :], moe_gain[...]).astype(jnp.bfloat16)
        return carry

    lax.fori_loop(0, tokens // ROW_TILE, normal_rows, 0)

    def column(row_data):
        return jnp.broadcast_to(row_data, (LANES, tokens)).T[:, 0:1]

    slot_rank = [near_rank(j) for j in range(half)]
    slot_rank += [far_rank(s // 2, s % 2) for s in range(half)]
    earlier = (
        lax.broadcasted_iota(jnp.int32, (tokens, tokens), 0)
        > lax.broadcasted_iota(jnp.int32, (tokens, tokens), 1)
    ).astype(jnp.float32).astype(jnp.bfloat16)
    lane = lax.broadcasted_iota(jnp.int32, (tokens, LANES), 1).astype(jnp.float32)

    def slots_of(block):
        chosen = index_ref[:, pl.ds(pl.multiple_of(block * tokens, tokens), tokens)]
        order = jnp.zeros(chosen.shape, jnp.float32)
        for s in range(1, n):
            order = order + jnp.where(chosen == slot_rank[s], float(s), 0.0)
        first, second = column(order[0:1, :]), column(order[1:2, :])
        hot_first = (lane == first).astype(jnp.float32)
        hot_second = (lane == second).astype(jnp.float32)
        before = jnp.dot(
            earlier,
            (hot_first + hot_second).astype(jnp.bfloat16),
            preferred_element_type=jnp.float32,
        )
        return (
            first * slots + jnp.sum(before * hot_first, axis=1, keepdims=True),
            second * slots + jnp.sum(before * hot_second, axis=1, keepdims=True),
        )

    def spread_of(pair, count):
        row_first = jnp.broadcast_to(pair[0], (tokens, LANES)).T[0:1, :]
        row_second = jnp.broadcast_to(pair[1], (tokens, LANES)).T[0:1, :]
        slot_row = lax.broadcasted_iota(jnp.int32, (count * slots, tokens), 0).astype(jnp.float32)
        return (
            jnp.where(slot_row == row_first, 1.0, 0.0) + jnp.where(slot_row == row_second, 1.0, 0.0)
        ).astype(jnp.bfloat16)

    def share_of(pair, weights, base, count):
        slot_lane = base * slots + lax.broadcasted_iota(
            jnp.int32, (tokens, count * slots), 1
        ).astype(jnp.float32)
        share = jnp.where(slot_lane == pair[0], column(weights[0:1, :]), 0.0) + jnp.where(
            slot_lane == pair[1], column(weights[1:2, :]), 0.0
        )
        high = share.astype(jnp.bfloat16)
        return high, (share - high.astype(jnp.float32)).astype(jnp.bfloat16)

    def weighed(shares, rows):
        return jnp.dot(shares[0], rows, preferred_element_type=jnp.float32) + jnp.dot(
            shares[1], rows, preferred_element_type=jnp.float32
        )

    pair = slots_of(t)
    spread = spread_of(pair, n)
    for c in range(0, width, COLS):
        rows = jnp.dot(spread, normal[:, c : c + COLS], preferred_element_type=jnp.float32)
        rows = rows.astype(jnp.bfloat16).reshape(n, slots, COLS)
        own[:, :, c : c + COLS] = rows
        gath[0, t, :, c : c + COLS] = rows[0]

    pl.semaphore_wait(barrier, len(greeted))
    fetches[1].wait()

    @pl.when(place < n * 4 - 1)
    def _():
        halo_copy.start()

    normal_y.start()
    weight_y.start()

    held = [(there, j) for j in range(2) for there in range(2)]

    @pl.when(outer == 0)
    def _():
        for there, j in held:
            send_far(there, j).start()

    for j in (1, 2, 3):
        send_near(j).start()

    @pl.when(outer == 1)
    def _():
        send_far(*held[0]).start()

    share_core(0, t).start()

    fetches[2].wait()

    @pl.when(place > 0)
    def _():
        conv_copy(halo, halo, 0, (e, core_peer)).wait_recv()

    @pl.when(place > 0)
    def _():
        pad[0:halo_rows, :] = halo[...].astype(jnp.float32)

    @pl.when(place == 0)
    def _():
        pad[0:halo_rows, :] = jnp.zeros((halo_rows, width), jnp.float32)

    pad[halo_rows:, :] = conv_in[...].astype(jnp.float32)

    def strip(c, carry):
        cols = pl.ds(pl.multiple_of(c * LANES, LANES), LANES)
        running = jnp.zeros((tokens, LANES), jnp.float32)
        for k in range(reach + 1):
            start = halo_rows - reach + k
            running = running + pad[pl.ds(start, tokens), cols] * taps[pl.ds(k, 1), cols]
        mixed[:, cols] = running
        return carry

    lax.fori_loop(0, width // LANES, strip, 0)

    def conv_rows(i, carry):
        rows = pl.ds(pl.multiple_of(i * ROW_TILE, ROW_TILE), ROW_TILE)
        conv_all[t, rows, :] = jax.nn.silu(layer_scale(mixed[rows, :], conv_gain[...])).astype(
            jnp.bfloat16
        )
        return carry

    lax.fori_loop(0, tokens // ROW_TILE, conv_rows, 0)
    conv_core.start()

    def relay(k):
        arrive(k).wait_recv()

        @pl.when(is_far(k))
        def _():
            share_y(k, t).start()

        share_core(k, t).start()

    relay(1)
    for p in range(CONV_PARTS // 2):
        conv_y(t, p).start()

    normal_y.wait_recv()
    pair_peer = slots_of(y_peer)
    spread_peer = spread_of(pair_peer, half)
    for c in range(0, width, COLS):
        rows = jnp.dot(spread_peer, normal_peer[:, c : c + COLS], preferred_element_type=jnp.float32)
        rows = rows.astype(jnp.bfloat16).reshape(half, slots, COLS)
        own_peer[:, :, c : c + COLS] = rows
        gath[0, y_peer, :, c : c + COLS] = rows[0]
    for j in (1, 2, 3):
        send_near_peer(j).start()

    @pl.when(outer == 1)
    def _():
        for there, j in held[1:]:
            send_far(there, j).start()

    forward_core(0, y_peer).start()
    relay(2)
    for p in range(CONV_PARTS // 2, CONV_PARTS):
        conv_y(t, p).start()
    for fetch in fetches[3:6]:
        fetch.wait()

    def meet_core(k):
        reduce_core(k, core_peer, 0).wait_recv()
        reduce_core(k, core_peer, 1).wait_recv()

        @pl.when(is_far(k))
        def _():
            pair_sum[k] = (
                part[k, y_peer].astype(jnp.float32) + from_core[1, k].astype(jnp.float32)
            ).astype(jnp.bfloat16)
            reduce_y(k).start()

        @pl.when((k > 1) & (k <= half))
        def _():
            result[k] = (
                part[k, t].astype(jnp.float32) + from_core[0, k].astype(jnp.float32)
            ).astype(jnp.bfloat16)
            return_near(k).start()
            result_peer[k] = (
                part[k, y_peer].astype(jnp.float32) + from_core[1, k].astype(jnp.float32)
            ).astype(jnp.bfloat16)
            return_near_peer(k).start()

        @pl.when(k == 0)
        def _():
            returned[0] = (
                part[0, t].astype(jnp.float32) + from_core[0, 0].astype(jnp.float32)
            ).astype(jnp.bfloat16)
            returned_peer[0] = (
                part[0, y_peer].astype(jnp.float32) + from_core[1, 0].astype(jnp.float32)
            ).astype(jnp.bfloat16)

    def meet_y(k):
        reduce_y(k).wait_recv()
        summed = part[k, t].astype(jnp.float32) + from_core[0, k].astype(jnp.float32)
        result[k] = (summed + from_y[k].astype(jnp.float32)).astype(jnp.bfloat16)
        return_far(k).start()

    def step(i, carry):
        share_core(i, core_peer).wait_recv()
        forward_core(i, diagonal).wait_recv()
        rows = gath[i].reshape(4 * slots, width)
        hidden = gated(rows, gate_w[...], up_w[...])
        for c in range(0, width, COLS):
            piece = jnp.dot(hidden, down_w[:, c : c + COLS], preferred_element_type=jnp.float32)
            part[i, :, :, c : c + COLS] = piece.astype(jnp.bfloat16).reshape(4, slots, COLS)
        reduce_core(i, diagonal, 1).start()
        reduce_core(i, core_peer, 0).start()

        @pl.when(i < n - 3)
        def _():
            relay(i + 3)

        @pl.when(i + 1 < n)
        def _():
            share_y(i + 1, y_peer).wait_recv()
            forward_core(i + 1, y_peer).start()

        meet_core(i)

        @pl.when(i == half)
        def _():
            for p in range(CONV_PARTS):
                conv_y(y_peer, p).wait_recv()
            conv_pass.start()
            meet_y(1)

        @pl.when(i == n - 1)
        def _():
            meet_y(n - 3)

        return carry

    lax.fori_loop(0, n, step, 0)
    meet_y(n - 2)

    for fetch in fetches[6:]:
        fetch.wait()
    conv_copy(conv_all.at[core_peer], conv_all.at[core_peer], 3, (e, core_peer)).wait_recv()
    conv_copy(conv_all.at[diagonal], conv_all.at[diagonal], 4, (e, core_peer)).wait_recv()

    for j in (1, 2, 3):
        remote(result.at[j], returned.at[j], 7, j, (e, core_peer)).wait_recv()
        remote(result.at[j], returned_peer.at[j], 8, j, (e, core_peer)).wait_recv()
    weight_y.wait_recv()
    peer_share = share_of(pair_peer, weight_peer, 0, half)
    for c in range(0, width, COLS):
        rows = returned_peer[:, :, c : c + COLS].reshape(half * slots, COLS)
        near_send[:, c : c + COLS] = weighed(peer_share, rows).astype(jnp.bfloat16)
    near_y.start()

    meet_y(n - 1)

    for q in range(4):
        conv_out[q * tokens : (q + 1) * tokens, :] = jnp.dot(
            conv_all[q], out_w[...], preferred_element_type=jnp.float32
        ).astype(jnp.bfloat16)

    shared = gated(normal[...], sh_gate[...], sh_up[...])
    near_share = share_of(pair, weight_ref, 0, half)
    for c in range(0, width, COLS):
        rows = returned[0:half, :, c : c + COLS].reshape(half * slots, COLS)
        piece = jnp.dot(shared, sh_down[:, c : c + COLS], preferred_element_type=jnp.float32)
        total[:, c : c + COLS] = piece + weighed(near_share, rows)

    far_share = share_of(pair, weight_ref, half, half)
    near_y.wait_recv()
    for s in range(half, n):
        remote(result.at[s], returned.at[s], 7, s, (e, core_peer)).wait_recv()
    for c in range(0, width, COLS):
        rows = returned[half:n, :, c : c + COLS].reshape(half * slots, COLS)
        piece = total[:, c : c + COLS] + near_recv[:, c : c + COLS].astype(jnp.float32)
        moe_out[:, c : c + COLS] = (piece + weighed(far_share, rows)).astype(jnp.bfloat16)

    @pl.when(place < n * 4 - 1)
    def _():
        halo_copy.wait_send()

    for copy in (normal_y, weight_y, conv_core, conv_pass, near_y):
        copy.wait_send()
    for p in range(CONV_PARTS):
        conv_y(t, p).wait_send()

    def drain(k, carry):
        @pl.when(k > 0)
        def _():
            arrive(k).wait_send()

        @pl.when(is_far(k))
        def _():
            share_y(k, t).wait_send()
            reduce_y(k).wait_send()

        @pl.when((k > 1) & (k <= half))
        def _():
            share_y(k, t).wait_send()
            return_near_peer(k).wait_send()

        @pl.when(k > 0)
        def _():
            remote(result.at[k], returned.at[k], 7, k, (e, core_peer)).wait_send()

        share_core(k, t).wait_send()
        forward_core(k, y_peer).wait_send()
        reduce_core(k, diagonal, 1).wait_send()
        reduce_core(k, core_peer, 0).wait_send()
        return carry

    lax.fori_loop(0, n, drain, 0)


def fused(
    conv_input,
    conv_kernel,
    conv_gain,
    out_weight,
    moe_input,
    moe_gain,
    expert_gate,
    expert_up,
    expert_down,
    shared_gate,
    shared_up,
    shared_down,
    expert_index,
    routing_weight,
):
    n = lax.axis_size("ep")
    parts = lax.axis_size("tp")
    tokens, width = moe_input.shape
    slots = 3 * tokens * routing_weight.shape[1] // (2 * n)
    hidden = expert_gate.shape[2]
    shared_hidden = shared_gate.shape[1]
    reach = conv_kernel.shape[0] - 1
    halo_rows = -(-reach // ROW_TILE) * ROW_TILE
    out_cols = out_weight.shape[1]
    bf16 = jnp.bfloat16
    chunk = (n, slots, width)
    half_chunk = (n // 2, slots, width)
    rows = (tokens, width)
    vmem = pl.BlockSpec(memory_space=pltpu.VMEM)
    hbm = pl.BlockSpec(memory_space=pl.ANY)
    return pl.pallas_call(
        functools.partial(fused_kernel, n, slots, reach),
        out_shape=(
            pltpu.VMEM((parts * tokens, out_cols), bf16),
            pltpu.VMEM(rows, bf16),
        ),
        in_specs=[hbm, hbm, vmem, hbm, hbm, vmem, hbm, hbm, hbm, hbm, hbm, hbm, vmem, vmem],
        out_specs=(vmem, vmem),
        scratch_shapes=[
            pltpu.VMEM(chunk, bf16),
            pltpu.VMEM(half_chunk, bf16),
            pltpu.VMEM((n, parts, slots, width), bf16),
            pltpu.VMEM((n, parts, slots, width), bf16),
            pltpu.VMEM((2,) + chunk, bf16),
            pltpu.VMEM(chunk, bf16),
            pltpu.VMEM(chunk, bf16),
            pltpu.VMEM(chunk, bf16),
            pltpu.VMEM(chunk, bf16),
            pltpu.VMEM(chunk, bf16),
            pltpu.VMEM(half_chunk, bf16),
            pltpu.VMEM(rows, bf16),
            pltpu.VMEM(rows, bf16),
            pltpu.VMEM((2, tokens), jnp.float32),
            pltpu.VMEM(rows, bf16),
            pltpu.VMEM(rows, bf16),
            pltpu.VMEM(rows, jnp.float32),
            pltpu.VMEM((halo_rows, width), bf16),
            pltpu.VMEM((halo_rows + tokens, width), jnp.float32),
            pltpu.VMEM(rows, jnp.float32),
            pltpu.VMEM((parts, tokens, width), bf16),
            pltpu.VMEM(rows, bf16),
            pltpu.VMEM((reach + 1, width), jnp.float32),
            pltpu.VMEM(rows, bf16),
            pltpu.VMEM((width, hidden), bf16),
            pltpu.VMEM((width, hidden), bf16),
            pltpu.VMEM((hidden, width), bf16),
            pltpu.VMEM((width, shared_hidden), bf16),
            pltpu.VMEM((width, shared_hidden), bf16),
            pltpu.VMEM((shared_hidden, width), bf16),
            pltpu.VMEM((width, out_cols), bf16),
            pltpu.SemaphoreType.DMA((10,)),
            pltpu.SemaphoreType.DMA((9, n)),
            pltpu.SemaphoreType.DMA((9, n)),
            pltpu.SemaphoreType.DMA((6 + CONV_PARTS,)),
            pltpu.SemaphoreType.DMA((6 + CONV_PARTS,)),
        ],
        compiler_params=pltpu.CompilerParams(
            collective_id=0, has_side_effects=True, vmem_limit_bytes=60 * 1024 * 1024
        ),
    )(
        conv_input,
        conv_kernel,
        conv_gain.reshape(1, width),
        out_weight,
        moe_input,
        moe_gain.reshape(1, width),
        expert_gate,
        expert_up,
        expert_down,
        shared_gate,
        shared_up,
        shared_down,
        expert_index.T,
        routing_weight.T,
    )


def fits_fused(args):
    n, parts = lax.axis_size("ep"), lax.axis_size("tp")
    conv_input, conv_kernel, moe_input = args[0], args[1], args[4]
    top_count = args[13].shape[1]
    tokens, width = moe_input.shape
    slots = 3 * tokens * top_count // (2 * n)
    return (
        parts == 4
        and top_count == 2
        and args[6].shape[0] == 1
        and conv_input.shape == moe_input.shape
        and conv_kernel.shape[0] - 1 <= tokens
        and tokens % LANES == 0
        and width % COLS == 0
        and slots % ROW_TILE == 0
        and slots >= ROW_TILE
        and n == 8
    )


def either(*args):
    return fused(*args) if fits_fused(args) else on_device(*args)


def solution(mesh):
    in_specs = (
        P(("ep", "tp"), None),
        P(),
        P(),
        P(None, "tp"),
        P(("ep", "tp"), None),
        P(),
        P("ep", None, "tp"),
        P("ep", None, "tp"),
        P("ep", "tp", None),
        P(),
        P(),
        P(),
        P("ep", None),
        P(("ep", "tp"), None),
    )
    out_specs = (P("ep", "tp"), P(("ep", "tp"), None))
    return jax.shard_map(
        either, mesh=mesh, in_specs=in_specs, out_specs=out_specs, check_vma=False
    )
```

```python
import functools

import jax
import jax.numpy as jnp
from jax import lax
from jax.experimental import pallas as pl
from jax.experimental.pallas import tpu as pltpu
from jax.sharding import PartitionSpec as P

NORM_EPS = 1e-05


def passed_along(block, axis, distance):
    devices = range(lax.axis_size(axis))
    route = [(i - distance, i) for i in devices if i - distance in devices]
    return lax.ppermute(block, axis, route)


def layer_scale(row_data, gain_vec):
    values = row_data.astype(jnp.float32)
    center = values - jnp.mean(values, axis=-1, keepdims=True)
    spread = jnp.mean(center * center, axis=-1, keepdims=True)
    return center * lax.rsqrt(spread + NORM_EPS) * gain_vec


def depthwise(padded, kernel, length):
    running = jnp.zeros((length, padded.shape[1]), jnp.float32)
    for offset in range(kernel.shape[0]):
        running = running + padded[offset : offset + length].astype(jnp.float32) * kernel[offset]
    return running


def slot_table(block_index, experts, slot_count):
    onehot = (
        block_index[:, :, None] == jnp.arange(experts, dtype=jnp.int32)[None, None, :]
    ).astype(jnp.int32)
    before = jnp.cumsum(onehot, axis=1) - onehot
    position = jnp.sum(before * onehot, axis=2)
    return block_index * slot_count + position


def fill_slots(row_data, entry_slot, top_count, total_slots):
    block_count = entry_slot.shape[0]
    entries = entry_slot.shape[1]
    block_ids = jnp.arange(block_count, dtype=jnp.int32)[:, None]
    source = jnp.arange(entries, dtype=jnp.int32)[None, :] // top_count
    slot_row = (
        jnp.zeros((block_count, total_slots), jnp.int32).at[block_ids, entry_slot].set(source)
    )
    filled = jnp.zeros((block_count, total_slots), jnp.int32).at[block_ids, entry_slot].set(1)
    picked = row_data[block_ids, slot_row]
    return jnp.where(filled[:, :, None] > 0, picked, jnp.zeros((), row_data.dtype))


def gated(row_data, gate_weight, up_weight):
    gate_proj = jnp.dot(row_data, gate_weight, preferred_element_type=jnp.float32)
    up_proj = jnp.dot(row_data, up_weight, preferred_element_type=jnp.float32)
    return (jax.nn.silu(gate_proj) * up_proj).astype(jnp.bfloat16)


def on_device(
    conv_input,
    conv_kernel,
    conv_gain,
    out_weight,
    moe_input,
    moe_gain,
    expert_gate,
    expert_up,
    expert_down,
    shared_gate,
    shared_up,
    shared_down,
    expert_index,
    routing_weight,
):
    reach = conv_kernel.shape[0] - 1
    length = conv_input.shape[0]
    halo_rows = passed_along(conv_input[length - reach :], ("ep", "tp"), 1)
    padded = jnp.concatenate([halo_rows, conv_input], axis=0)
    mixed_rows = depthwise(padded, conv_kernel, length)
    normed = jax.nn.silu(layer_scale(mixed_rows, conv_gain)).astype(jnp.bfloat16)
    conv_out = jnp.dot(
        lax.all_gather(normed, "tp", axis=0, tiled=True),
        out_weight,
        preferred_element_type=jnp.float32,
    ).astype(jnp.bfloat16)
    tp_parts = lax.axis_size("tp")
    tp_index = lax.axis_index("tp")
    ep_ranks = lax.axis_size("ep")
    tok_count = moe_input.shape[0]
    top_count = routing_weight.shape[1]
    model_width = moe_input.shape[1]
    experts = ep_ranks * expert_gate.shape[0]
    slot_count = 3 * tok_count * top_count // (2 * experts)
    total_slots = experts * slot_count
    normal = layer_scale(moe_input, moe_gain).astype(jnp.bfloat16)
    group_slots = slot_table(
        expert_index.reshape(tp_parts, tok_count * top_count), experts, slot_count
    )
    own_slots = lax.dynamic_index_in_dim(group_slots, tp_index, 0, keepdims=True)
    gate_local = expert_gate[0]
    up_local = expert_up[0]
    down_local = expert_down[0]
    own_rows = fill_slots(normal[None], own_slots, top_count, total_slots)
    own_rows = own_rows.reshape(ep_ranks, slot_count, model_width)
    arrived = lax.all_to_all(own_rows, "ep", split_axis=0, concat_axis=0, tiled=True)
    hidden = gated(
        lax.all_gather(
            arrived.reshape(ep_ranks * slot_count, model_width), "tp", axis=0, tiled=True
        ),
        gate_local,
        up_local,
    )
    summed = lax.psum_scatter(
        jnp.dot(hidden, down_local, preferred_element_type=jnp.float32).astype(jnp.bfloat16),
        "tp",
        scatter_dimension=0,
        tiled=True,
    )
    returned = lax.all_to_all(
        summed.reshape(ep_ranks, slot_count, model_width),
        "ep",
        split_axis=0,
        concat_axis=0,
        tiled=True,
    )
    picked = returned.reshape(total_slots, model_width)[own_slots[0]]
    picked = picked.reshape(tok_count, top_count, model_width).astype(jnp.float32)
    routed = jnp.sum(picked * routing_weight[:, :, None], axis=1)
    shared_hidden = gated(normal, shared_gate, shared_up)
    shared_part = jnp.dot(shared_hidden, shared_down, preferred_element_type=jnp.float32)
    moe_out = (shared_part + routed).astype(jnp.bfloat16)
    return (conv_out, moe_out)


LANES = 128
ROW_TILE = 16
COLS = 512
CONV_PARTS = 4
MESH = pl.DeviceIdType.MESH


def fused_kernel(
    n,
    slots,
    reach,
    conv_hbm,
    taps_hbm,
    conv_gain,
    out_w_hbm,
    moe_hbm,
    moe_gain,
    gate_hbm,
    up_hbm,
    down_hbm,
    sh_gate_hbm,
    sh_up_hbm,
    sh_down_hbm,
    index_ref,
    weight_ref,
    conv_out,
    moe_out,
    own,
    own_peer,
    gath,
    part,
    from_core,
    pair_sum,
    from_y,
    result,
    result_peer,
    returned,
    returned_peer,
    normal,
    normal_peer,
    weight_peer,
    near_send,
    near_recv,
    total,
    halo,
    pad,
    mixed,
    conv_all,
    conv_in,
    taps,
    moe_in,
    gate_w,
    up_w,
    down_w,
    sh_gate,
    sh_up,
    sh_down,
    out_w,
    local_sem,
    chunk_send,
    chunk_recv,
    conv_send,
    conv_recv,
):
    tokens, width = moe_hbm.shape
    e = lax.axis_index("ep")
    t = lax.axis_index("tp")
    core = lax.rem(t, 2)
    row = t // 2
    core_peer = row * 2 + (1 - core)
    y_peer = (1 - row) * 2 + core
    diagonal = (1 - row) * 2 + (1 - core)
    place = e * 4 + t
    after = lax.rem(place + 1, n * 4)
    ahead = lax.rem(place + n * 4 - 1, n * 4)
    halo_rows = halo.shape[0]
    half = n // 2
    side = e // half
    deep = lax.rem(e, half) // 2
    across = lax.rem(e, 2)
    outer = side * deep + (1 - side) * (1 - deep)
    conv_cut = tokens // CONV_PARTS

    fetches = [
        pltpu.make_async_copy(src, dst, local_sem.at[i])
        for i, (src, dst) in enumerate(
            (
                (moe_hbm, moe_in),
                (conv_hbm, conv_in),
                (taps_hbm, taps),
                (gate_hbm.at[0], gate_w),
                (up_hbm.at[0], up_w),
                (down_hbm.at[0], down_w),
                (sh_gate_hbm, sh_gate),
                (sh_up_hbm, sh_up),
                (sh_down_hbm, sh_down),
                (out_w_hbm, out_w),
            )
        )
    ]
    for fetch in fetches:
        fetch.start()

    barrier = pltpu.get_barrier_semaphore()
    greeted = [(lax.rem(e + k, n), t) for k in range(1, n)]
    greeted += [(e, core_peer), (e, y_peer)]
    greeted += [(after // 4, lax.rem(after, 4)), (ahead // 4, lax.rem(ahead, 4))]
    for device in greeted:
        pl.semaphore_signal(barrier, inc=1, device_id=device, device_id_type=MESH)

    def flip(a, b):
        return a + b - 2 * a * b

    def near_rank(j):
        return side * half + 2 * flip(deep, j // 2) + flip(across, lax.rem(j, 2))

    def far_rank(there, j):
        return (1 - side) * half + 2 * there + flip(across, j)

    def near_item(j):
        return 0 if j == 0 else j + 1

    def is_far(k):
        return (k == 1) | (k > half)

    def far_parts(k):
        v = (k // (half + 1)) * (k - half)
        q = (v + 1) // 2
        from_outer = (1 - outer) * (v // 2) + outer * (1 - q * (2 - q))
        return from_outer, (1 - outer) * lax.rem(v, 2) + outer * (v // 2)

    def packed(order):
        return sum(item * n**place for place, item in enumerate(order))

    item_order = (1 - outer) * packed((0, 1, 5, 2, 3, 4, 6, 7)) + outer * packed(
        (0, 1, 2, 5, 3, 6, 4, 7)
    )

    def remote(src, dst, kind, k, device, k_there=None):
        return pltpu.make_async_remote_copy(
            src_ref=src,
            dst_ref=dst,
            send_sem=chunk_send.at[kind, k],
            recv_sem=chunk_recv.at[kind, k if k_there is None else k_there],
            device_id=device,
            device_id_type=MESH,
        )

    def conv_copy(src, dst, kind, device):
        return pltpu.make_async_remote_copy(
            src_ref=src,
            dst_ref=dst,
            send_sem=conv_send.at[kind],
            recv_sem=conv_recv.at[kind],
            device_id=device,
            device_id_type=MESH,
        )

    def send_near(j):
        k = near_item(j)
        return remote(own.at[j], gath.at[k, t], 0, j, (near_rank(j), t), k)

    def send_near_peer(j):
        k = near_item(j)
        return remote(own_peer.at[j], gath.at[k, y_peer], 1, k, (near_rank(j), t))

    def send_far(to_outer, j):
        there = (1 - side) * to_outer + side * (1 - to_outer)
        if to_outer:
            v = (1 - outer) * (1 + j) + outer * 3 * j
        else:
            v = 2 * outer + j
        k = 1 + v + 3 * ((v + 2) // 3)
        s = half + 2 * there + j
        return remote(own.at[s], gath.at[k, t], 0, s, (far_rank(there, j), t), k)

    def arrive(k):
        return remote(own.at[k], gath.at[k, t], 0, k, (e, core_peer))

    def share_core(k, q):
        return remote(gath.at[k, q], gath.at[k, q], 2, k, (e, core_peer))

    def share_y(k, q):
        return remote(gath.at[k, q], gath.at[k, q], 1, k, (e, y_peer))

    def forward_core(k, q):
        return remote(gath.at[k, q], gath.at[k, q], 3, k, (e, core_peer))

    def reduce_core(k, q, which):
        return remote(part.at[k, q], from_core.at[which, k], 4 + which, k, (e, core_peer))

    def reduce_y(k):
        return remote(pair_sum.at[k], from_y.at[k], 6, k, (e, y_peer))

    def return_near(k):
        j = k - 1
        return remote(result.at[k], returned.at[j], 7, k, (near_rank(j), t), j)

    def return_near_peer(k):
        j = k - 1
        return remote(result_peer.at[k], returned_peer.at[j], 8, k, (near_rank(j), t), j)

    def return_far(k):
        m, j = far_parts(k)
        there = m * (1 - side) + (1 - m) * side
        s = half + 2 * deep + j
        return remote(result.at[k], returned.at[s], 7, k, (far_rank(there, j), t), s)

    normal_y = conv_copy(normal, normal_peer, 1, (e, y_peer))
    weight_y = conv_copy(weight_ref, weight_peer, 2, (e, y_peer))
    halo_copy = conv_copy(
        conv_in.at[pl.ds(tokens - halo_rows, halo_rows)],
        halo,
        0,
        (after // 4, lax.rem(after, 4)),
    )
    conv_core = conv_copy(conv_all.at[t], conv_all.at[t], 3, (e, core_peer))
    conv_pass = conv_copy(conv_all.at[y_peer], conv_all.at[y_peer], 4, (e, core_peer))
    near_y = conv_copy(near_send, near_recv, 5, (e, y_peer))

    def conv_y(q, p):
        block = conv_all.at[q, pl.ds(p * conv_cut, conv_cut)]
        return conv_copy(block, block, 6 + p, (e, y_peer))

    fetches[0].wait()

    def normal_rows(i, carry):
        rows = pl.ds(pl.multiple_of(i * ROW_TILE, ROW_TILE), ROW_TILE)
        normal[rows, :] = layer_scale(moe_in[rows, :], moe_gain[...]).astype(jnp.bfloat16)
        return carry

    lax.fori_loop(0, tokens // ROW_TILE, normal_rows, 0)

    def column(row_data):
        return jnp.broadcast_to(row_data, (LANES, tokens)).T[:, 0:1]

    slot_rank = [near_rank(j) for j in range(half)]
    slot_rank += [far_rank(s // 2, s % 2) for s in range(half)]
    earlier = (
        lax.broadcasted_iota(jnp.int32, (tokens, tokens), 0)
        > lax.broadcasted_iota(jnp.int32, (tokens, tokens), 1)
    ).astype(jnp.float32).astype(jnp.bfloat16)
    lane = lax.broadcasted_iota(jnp.int32, (tokens, LANES), 1).astype(jnp.float32)

    def slots_of(block):
        chosen = index_ref[:, pl.ds(pl.multiple_of(block * tokens, tokens), tokens)]
        order = jnp.zeros(chosen.shape, jnp.float32)
        for s in range(1, n):
            order = order + jnp.where(chosen == slot_rank[s], float(s), 0.0)
        first, second = column(order[0:1, :]), column(order[1:2, :])
        hot_first = (lane == first).astype(jnp.float32)
        hot_second = (lane == second).astype(jnp.float32)
        before = jnp.dot(
            earlier,
            (hot_first + hot_second).astype(jnp.bfloat16),
            preferred_element_type=jnp.float32,
        )
        return (
            first * slots + jnp.sum(before * hot_first, axis=1, keepdims=True),
            second * slots + jnp.sum(before * hot_second, axis=1, keepdims=True),
        )

    def spread_of(pair, count):
        row_first = jnp.broadcast_to(pair[0], (tokens, LANES)).T[0:1, :]
        row_second = jnp.broadcast_to(pair[1], (tokens, LANES)).T[0:1, :]
        slot_row = lax.broadcasted_iota(jnp.int32, (count * slots, tokens), 0).astype(jnp.float32)
        return (
            jnp.where(slot_row == row_first, 1.0, 0.0) + jnp.where(slot_row == row_second, 1.0, 0.0)
        ).astype(jnp.bfloat16)

    def share_of(pair, weights, base, count):
        slot_lane = base * slots + lax.broadcasted_iota(
            jnp.int32, (tokens, count * slots), 1
        ).astype(jnp.float32)
        share = jnp.where(slot_lane == pair[0], column(weights[0:1, :]), 0.0) + jnp.where(
            slot_lane == pair[1], column(weights[1:2, :]), 0.0
        )
        high = share.astype(jnp.bfloat16)
        return high, (share - high.astype(jnp.float32)).astype(jnp.bfloat16)

    def weighed(shares, rows):
        return jnp.dot(shares[0], rows, preferred_element_type=jnp.float32) + jnp.dot(
            shares[1], rows, preferred_element_type=jnp.float32
        )

    pl.semaphore_wait(barrier, len(greeted))
    fetches[1].wait()

    @pl.when(place < n * 4 - 1)
    def _():
        halo_copy.start()

    normal_y.start()
    weight_y.start()

    pair = slots_of(t)
    spread = spread_of(pair, n)
    for c in range(0, width, COLS):
        rows = jnp.dot(spread, normal[:, c : c + COLS], preferred_element_type=jnp.float32)
        rows = rows.astype(jnp.bfloat16).reshape(n, slots, COLS)
        own[:, :, c : c + COLS] = rows
        gath[0, t, :, c : c + COLS] = rows[0]

    @pl.when(outer == 0)
    def _():
        send_far(0, 0).start()
        send_far(0, 1).start()

    for j in (2, 3, 1):
        send_near(j).start()

    @pl.when(outer == 1)
    def _():
        send_far(1, 0).start()

    share_core(0, t).start()

    fetches[2].wait()

    @pl.when(place > 0)
    def _():
        conv_copy(halo, halo, 0, (e, core_peer)).wait_recv()

    @pl.when(place > 0)
    def _():
        pad[0:halo_rows, :] = halo[...].astype(jnp.float32)

    @pl.when(place == 0)
    def _():
        pad[0:halo_rows, :] = jnp.zeros((halo_rows, width), jnp.float32)

    pad[halo_rows:, :] = conv_in[...].astype(jnp.float32)

    def strip(c, carry):
        cols = pl.ds(pl.multiple_of(c * LANES, LANES), LANES)
        running = jnp.zeros((tokens, LANES), jnp.float32)
        for k in range(reach + 1):
            start = halo_rows - reach + k
            running = running + pad[pl.ds(start, tokens), cols] * taps[pl.ds(k, 1), cols]
        mixed[:, cols] = running
        return carry

    lax.fori_loop(0, width // LANES, strip, 0)

    def conv_rows(i, carry):
        rows = pl.ds(pl.multiple_of(i * ROW_TILE, ROW_TILE), ROW_TILE)
        conv_all[t, rows, :] = jax.nn.silu(layer_scale(mixed[rows, :], conv_gain[...])).astype(
            jnp.bfloat16
        )
        return carry

    lax.fori_loop(0, tokens // ROW_TILE, conv_rows, 0)
    conv_core.start()

    def relay(k):
        arrive(k).wait_recv()

        @pl.when(is_far(k))
        def _():
            share_y(k, t).start()

        share_core(k, t).start()

    @pl.when(outer == 0)
    def _():
        send_far(1, 0).start()
        relay(1)

    @pl.when(outer == 1)
    def _():
        for p in range(CONV_PARTS - 1):
            conv_y(t, p).start()

    normal_y.wait_recv()
    pair_peer = slots_of(y_peer)
    spread_peer = spread_of(pair_peer, half)
    for c in range(0, width, COLS):
        rows = jnp.dot(spread_peer, normal_peer[:, c : c + COLS], preferred_element_type=jnp.float32)
        rows = rows.astype(jnp.bfloat16).reshape(half, slots, COLS)
        own_peer[:, :, c : c + COLS] = rows
        gath[0, y_peer, :, c : c + COLS] = rows[0]
    @pl.when(outer == 1)
    def _():
        send_far(1, 1).start()

    for j in (2, 3, 1):
        send_near_peer(j).start()

    @pl.when(outer == 0)
    def _():
        send_far(1, 1).start()

    @pl.when(outer == 1)
    def _():
        send_far(0, 0).start()
        send_far(0, 1).start()

    forward_core(0, y_peer).start()
    relay(2)
    relay(3)
    relay(4)
    for fetch in fetches[3:6]:
        fetch.wait()

    def meet_core(k):
        reduce_core(k, core_peer, 0).wait_recv()
        reduce_core(k, core_peer, 1).wait_recv()

        @pl.when(is_far(k))
        def _():
            pair_sum[k] = (
                part[k, y_peer].astype(jnp.float32) + from_core[1, k].astype(jnp.float32)
            ).astype(jnp.bfloat16)
            reduce_y(k).start()

        @pl.when((k > 1) & (k <= half))
        def _():
            result[k] = (
                part[k, t].astype(jnp.float32) + from_core[0, k].astype(jnp.float32)
            ).astype(jnp.bfloat16)
            return_near(k).start()
            result_peer[k] = (
                part[k, y_peer].astype(jnp.float32) + from_core[1, k].astype(jnp.float32)
            ).astype(jnp.bfloat16)
            return_near_peer(k).start()

        @pl.when(k == 0)
        def _():
            returned[0] = (
                part[0, t].astype(jnp.float32) + from_core[0, 0].astype(jnp.float32)
            ).astype(jnp.bfloat16)
            returned_peer[0] = (
                part[0, y_peer].astype(jnp.float32) + from_core[1, 0].astype(jnp.float32)
            ).astype(jnp.bfloat16)

    def meet_y(k):
        reduce_y(k).wait_recv()
        summed = part[k, t].astype(jnp.float32) + from_core[0, k].astype(jnp.float32)
        result[k] = (summed + from_y[k].astype(jnp.float32)).astype(jnp.bfloat16)
        return_far(k).start()

    def step(i, carry):
        k = lax.rem(carry, n)
        later = lax.rem(carry // n, n)
        share_core(k, core_peer).wait_recv()
        forward_core(k, diagonal).wait_recv()
        rows = gath[k].reshape(4 * slots, width)
        hidden = gated(rows, gate_w[...], up_w[...])
        for c in range(0, width, COLS):
            piece = jnp.dot(hidden, down_w[:, c : c + COLS], preferred_element_type=jnp.float32)
            part[k, :, :, c : c + COLS] = piece.astype(jnp.bfloat16).reshape(4, slots, COLS)
        reduce_core(k, diagonal, 1).start()
        reduce_core(k, core_peer, 0).start()

        @pl.when((i == 0) & (outer == 1))
        def _():
            relay(1)
            conv_y(t, CONV_PARTS - 1).start()

        @pl.when(i == outer)
        def _():
            relay(5)

        @pl.when((i == 0) & (outer == 0))
        def _():
            for p in range(CONV_PARTS // 2):
                conv_y(t, p).start()

        @pl.when((i == 2) & (outer == 1))
        def _():
            relay(6)
            relay(7)

        meet_first = (i == n - 1) | ((outer == 0) & (i >= 4)) | ((outer == 1) & (lax.rem(i, 2) == 0) & (i < 6))

        @pl.when(meet_first)
        def _():
            meet_core(k)

        @pl.when(i == 4)
        def _():
            meet_y(1)

        @pl.when((i == 5) & (outer == 0))
        def _():
            relay(6)
            meet_y(5)
            relay(7)

        @pl.when((i == 7) & (outer == 1))
        def _():
            meet_y(5)

        @pl.when(i + 1 < n)
        def _():
            share_y(later, y_peer).wait_recv()
            forward_core(later, y_peer).start()

        @pl.when(jnp.logical_not(meet_first))
        def _():
            meet_core(k)

        @pl.when((i == 2) & (outer == 0))
        def _():
            conv_y(t, 2).start()

        return carry // n

    lax.fori_loop(0, n, step, item_order)

    @pl.when(outer == 0)
    def _():
        conv_y(t, CONV_PARTS - 1).start()

    meet_y(6)

    meet_y(7)
    for j in (1, 2, 3):
        remote(result.at[j], returned.at[j], 7, j, (e, core_peer)).wait_recv()
        remote(result.at[j], returned_peer.at[j], 8, j, (e, core_peer)).wait_recv()
    weight_y.wait_recv()
    peer_share = share_of(pair_peer, weight_peer, 0, half)
    for c in range(0, width, COLS):
        rows = returned_peer[:, :, c : c + COLS].reshape(half * slots, COLS)
        near_send[:, c : c + COLS] = weighed(peer_share, rows).astype(jnp.bfloat16)
    near_y.start()


    for p in range(CONV_PARTS):
        conv_y(y_peer, p).wait_recv()
    conv_pass.start()

    for fetch in fetches[6:]:
        fetch.wait()
    conv_copy(conv_all.at[core_peer], conv_all.at[core_peer], 3, (e, core_peer)).wait_recv()
    conv_copy(conv_all.at[diagonal], conv_all.at[diagonal], 4, (e, core_peer)).wait_recv()

    for q in range(4):
        conv_out[q * tokens : (q + 1) * tokens, :] = jnp.dot(
            conv_all[q], out_w[...], preferred_element_type=jnp.float32
        ).astype(jnp.bfloat16)

    shared = gated(normal[...], sh_gate[...], sh_up[...])
    near_share = share_of(pair, weight_ref, 0, half)
    for c in range(0, width, COLS):
        rows = returned[0:half, :, c : c + COLS].reshape(half * slots, COLS)
        piece = jnp.dot(shared, sh_down[:, c : c + COLS], preferred_element_type=jnp.float32)
        total[:, c : c + COLS] = piece + weighed(near_share, rows)

    far_share = share_of(pair, weight_ref, half, half)
    near_y.wait_recv()
    for s in range(half, n):
        remote(result.at[s], returned.at[s], 7, s, (e, core_peer)).wait_recv()
    for c in range(0, width, COLS):
        rows = returned[half:n, :, c : c + COLS].reshape(half * slots, COLS)
        piece = total[:, c : c + COLS] + near_recv[:, c : c + COLS].astype(jnp.float32)
        moe_out[:, c : c + COLS] = (piece + weighed(far_share, rows)).astype(jnp.bfloat16)

    @pl.when(place < n * 4 - 1)
    def _():
        halo_copy.wait_send()

    for copy in (normal_y, weight_y, conv_core, conv_pass, near_y):
        copy.wait_send()
    for p in range(CONV_PARTS):
        conv_y(t, p).wait_send()

    def drain(k, carry):
        @pl.when(k > 0)
        def _():
            arrive(k).wait_send()

        @pl.when(is_far(k))
        def _():
            share_y(k, t).wait_send()
            reduce_y(k).wait_send()

        @pl.when((k > 1) & (k <= half))
        def _():
            share_y(k, t).wait_send()
            return_near_peer(k).wait_send()

        @pl.when(k > 0)
        def _():
            remote(result.at[k], returned.at[k], 7, k, (e, core_peer)).wait_send()

        share_core(k, t).wait_send()
        forward_core(k, y_peer).wait_send()
        reduce_core(k, diagonal, 1).wait_send()
        reduce_core(k, core_peer, 0).wait_send()
        return carry

    lax.fori_loop(0, n, drain, 0)


def fused(
    conv_input,
    conv_kernel,
    conv_gain,
    out_weight,
    moe_input,
    moe_gain,
    expert_gate,
    expert_up,
    expert_down,
    shared_gate,
    shared_up,
    shared_down,
    expert_index,
    routing_weight,
):
    n = lax.axis_size("ep")
    parts = lax.axis_size("tp")
    tokens, width = moe_input.shape
    slots = 3 * tokens * routing_weight.shape[1] // (2 * n)
    hidden = expert_gate.shape[2]
    shared_hidden = shared_gate.shape[1]
    reach = conv_kernel.shape[0] - 1
    halo_rows = -(-reach // ROW_TILE) * ROW_TILE
    out_cols = out_weight.shape[1]
    bf16 = jnp.bfloat16
    chunk = (n, slots, width)
    half_chunk = (n // 2, slots, width)
    rows = (tokens, width)
    vmem = pl.BlockSpec(memory_space=pltpu.VMEM)
    hbm = pl.BlockSpec(memory_space=pl.ANY)
    return pl.pallas_call(
        functools.partial(fused_kernel, n, slots, reach),
        out_shape=(
            pltpu.VMEM((parts * tokens, out_cols), bf16),
            pltpu.VMEM(rows, bf16),
        ),
        in_specs=[hbm, hbm, vmem, hbm, hbm, vmem, hbm, hbm, hbm, hbm, hbm, hbm, vmem, vmem],
        out_specs=(vmem, vmem),
        scratch_shapes=[
            pltpu.VMEM(chunk, bf16),
            pltpu.VMEM(half_chunk, bf16),
            pltpu.VMEM((n, parts, slots, width), bf16),
            pltpu.VMEM((n, parts, slots, width), bf16),
            pltpu.VMEM((2,) + chunk, bf16),
            pltpu.VMEM(chunk, bf16),
            pltpu.VMEM(chunk, bf16),
            pltpu.VMEM(chunk, bf16),
            pltpu.VMEM(chunk, bf16),
            pltpu.VMEM(chunk, bf16),
            pltpu.VMEM(half_chunk, bf16),
            pltpu.VMEM(rows, bf16),
            pltpu.VMEM(rows, bf16),
            pltpu.VMEM((2, tokens), jnp.float32),
            pltpu.VMEM(rows, bf16),
            pltpu.VMEM(rows, bf16),
            pltpu.VMEM(rows, jnp.float32),
            pltpu.VMEM((halo_rows, width), bf16),
            pltpu.VMEM((halo_rows + tokens, width), jnp.float32),
            pltpu.VMEM(rows, jnp.float32),
            pltpu.VMEM((parts, tokens, width), bf16),
            pltpu.VMEM(rows, bf16),
            pltpu.VMEM((reach + 1, width), jnp.float32),
            pltpu.VMEM(rows, bf16),
            pltpu.VMEM((width, hidden), bf16),
            pltpu.VMEM((width, hidden), bf16),
            pltpu.VMEM((hidden, width), bf16),
            pltpu.VMEM((width, shared_hidden), bf16),
            pltpu.VMEM((width, shared_hidden), bf16),
            pltpu.VMEM((shared_hidden, width), bf16),
            pltpu.VMEM((width, out_cols), bf16),
            pltpu.SemaphoreType.DMA((10,)),
            pltpu.SemaphoreType.DMA((9, n)),
            pltpu.SemaphoreType.DMA((9, n)),
            pltpu.SemaphoreType.DMA((6 + CONV_PARTS,)),
            pltpu.SemaphoreType.DMA((6 + CONV_PARTS,)),
        ],
        compiler_params=pltpu.CompilerParams(
            collective_id=0, has_side_effects=True, vmem_limit_bytes=60 * 1024 * 1024
        ),
    )(
        conv_input,
        conv_kernel,
        conv_gain.reshape(1, width),
        out_weight,
        moe_input,
        moe_gain.reshape(1, width),
        expert_gate,
        expert_up,
        expert_down,
        shared_gate,
        shared_up,
        shared_down,
        expert_index.T,
        routing_weight.T,
    )


def fits_fused(args):
    n, parts = lax.axis_size("ep"), lax.axis_size("tp")
    conv_input, conv_kernel, moe_input = args[0], args[1], args[4]
    top_count = args[13].shape[1]
    tokens, width = moe_input.shape
    slots = 3 * tokens * top_count // (2 * n)
    return (
        parts == 4
        and top_count == 2
        and args[6].shape[0] == 1
        and conv_input.shape == moe_input.shape
        and conv_kernel.shape[0] - 1 <= tokens
        and tokens % LANES == 0
        and width % COLS == 0
        and slots % ROW_TILE == 0
        and slots >= ROW_TILE
        and n == 8
    )


def either(*args):
    return fused(*args) if fits_fused(args) else on_device(*args)


def solution(mesh):
    in_specs = (
        P(("ep", "tp"), None),
        P(),
        P(),
        P(None, "tp"),
        P(("ep", "tp"), None),
        P(),
        P("ep", None, "tp"),
        P("ep", None, "tp"),
        P("ep", "tp", None),
        P(),
        P(),
        P(),
        P("ep", None),
        P(("ep", "tp"), None),
    )
    out_specs = (P("ep", "tp"), P(("ep", "tp"), None))
    return jax.shard_map(
        either, mesh=mesh, in_specs=in_specs, out_specs=out_specs, check_vma=False
    )
```

```python
import functools

import jax
import jax.numpy as jnp
from jax import lax
from jax.experimental import pallas as pl
from jax.experimental.pallas import tpu as pltpu
from jax.sharding import PartitionSpec as P

NORM_EPS = 1e-05


def passed_along(block, axis, distance):
    devices = range(lax.axis_size(axis))
    route = [(i - distance, i) for i in devices if i - distance in devices]
    return lax.ppermute(block, axis, route)


def layer_scale(row_data, gain_vec):
    values = row_data.astype(jnp.float32)
    center = values - jnp.mean(values, axis=-1, keepdims=True)
    spread = jnp.mean(center * center, axis=-1, keepdims=True)
    return center * lax.rsqrt(spread + NORM_EPS) * gain_vec


def depthwise(padded, kernel, length):
    running = jnp.zeros((length, padded.shape[1]), jnp.float32)
    for offset in range(kernel.shape[0]):
        running = running + padded[offset : offset + length].astype(jnp.float32) * kernel[offset]
    return running


def slot_table(block_index, experts, slot_count):
    onehot = (
        block_index[:, :, None] == jnp.arange(experts, dtype=jnp.int32)[None, None, :]
    ).astype(jnp.int32)
    before = jnp.cumsum(onehot, axis=1) - onehot
    position = jnp.sum(before * onehot, axis=2)
    return block_index * slot_count + position


def fill_slots(row_data, entry_slot, top_count, total_slots):
    block_count = entry_slot.shape[0]
    entries = entry_slot.shape[1]
    block_ids = jnp.arange(block_count, dtype=jnp.int32)[:, None]
    source = jnp.arange(entries, dtype=jnp.int32)[None, :] // top_count
    slot_row = (
        jnp.zeros((block_count, total_slots), jnp.int32).at[block_ids, entry_slot].set(source)
    )
    filled = jnp.zeros((block_count, total_slots), jnp.int32).at[block_ids, entry_slot].set(1)
    picked = row_data[block_ids, slot_row]
    return jnp.where(filled[:, :, None] > 0, picked, jnp.zeros((), row_data.dtype))


def gated(row_data, gate_weight, up_weight):
    gate_proj = jnp.dot(row_data, gate_weight, preferred_element_type=jnp.float32)
    up_proj = jnp.dot(row_data, up_weight, preferred_element_type=jnp.float32)
    return (jax.nn.silu(gate_proj) * up_proj).astype(jnp.bfloat16)


def on_device(
    conv_input,
    conv_kernel,
    conv_gain,
    out_weight,
    moe_input,
    moe_gain,
    expert_gate,
    expert_up,
    expert_down,
    shared_gate,
    shared_up,
    shared_down,
    expert_index,
    routing_weight,
):
    reach = conv_kernel.shape[0] - 1
    length = conv_input.shape[0]
    halo_rows = passed_along(conv_input[length - reach :], ("ep", "tp"), 1)
    padded = jnp.concatenate([halo_rows, conv_input], axis=0)
    mixed_rows = depthwise(padded, conv_kernel, length)
    normed = jax.nn.silu(layer_scale(mixed_rows, conv_gain)).astype(jnp.bfloat16)
    conv_out = jnp.dot(
        lax.all_gather(normed, "tp", axis=0, tiled=True),
        out_weight,
        preferred_element_type=jnp.float32,
    ).astype(jnp.bfloat16)
    tp_parts = lax.axis_size("tp")
    tp_index = lax.axis_index("tp")
    ep_ranks = lax.axis_size("ep")
    tok_count = moe_input.shape[0]
    top_count = routing_weight.shape[1]
    model_width = moe_input.shape[1]
    experts = ep_ranks * expert_gate.shape[0]
    slot_count = 3 * tok_count * top_count // (2 * experts)
    total_slots = experts * slot_count
    normal = layer_scale(moe_input, moe_gain).astype(jnp.bfloat16)
    group_slots = slot_table(
        expert_index.reshape(tp_parts, tok_count * top_count), experts, slot_count
    )
    own_slots = lax.dynamic_index_in_dim(group_slots, tp_index, 0, keepdims=True)
    gate_local = expert_gate[0]
    up_local = expert_up[0]
    down_local = expert_down[0]
    own_rows = fill_slots(normal[None], own_slots, top_count, total_slots)
    own_rows = own_rows.reshape(ep_ranks, slot_count, model_width)
    arrived = lax.all_to_all(own_rows, "ep", split_axis=0, concat_axis=0, tiled=True)
    hidden = gated(
        lax.all_gather(
            arrived.reshape(ep_ranks * slot_count, model_width), "tp", axis=0, tiled=True
        ),
        gate_local,
        up_local,
    )
    summed = lax.psum_scatter(
        jnp.dot(hidden, down_local, preferred_element_type=jnp.float32).astype(jnp.bfloat16),
        "tp",
        scatter_dimension=0,
        tiled=True,
    )
    returned = lax.all_to_all(
        summed.reshape(ep_ranks, slot_count, model_width),
        "ep",
        split_axis=0,
        concat_axis=0,
        tiled=True,
    )
    picked = returned.reshape(total_slots, model_width)[own_slots[0]]
    picked = picked.reshape(tok_count, top_count, model_width).astype(jnp.float32)
    routed = jnp.sum(picked * routing_weight[:, :, None], axis=1)
    shared_hidden = gated(normal, shared_gate, shared_up)
    shared_part = jnp.dot(shared_hidden, shared_down, preferred_element_type=jnp.float32)
    moe_out = (shared_part + routed).astype(jnp.bfloat16)
    return (conv_out, moe_out)


LANES = 128
ROW_TILE = 16
COLS = 512
CONV_PARTS = 4
MESH = pl.DeviceIdType.MESH


def fused_kernel(
    n,
    slots,
    reach,
    conv_hbm,
    taps_hbm,
    conv_gain,
    out_w_hbm,
    moe_hbm,
    moe_gain,
    gate_hbm,
    up_hbm,
    down_hbm,
    sh_gate_hbm,
    sh_up_hbm,
    sh_down_hbm,
    index_ref,
    weight_ref,
    conv_out,
    moe_out,
    own,
    own_peer,
    gath,
    part,
    from_core,
    pair_sum,
    from_y,
    result,
    result_peer,
    returned,
    returned_peer,
    normal,
    normal_peer,
    weight_peer,
    near_send,
    near_recv,
    total,
    halo,
    pad,
    mixed,
    conv_all,
    conv_in,
    taps,
    moe_in,
    gate_w,
    up_w,
    down_w,
    sh_gate,
    sh_up,
    sh_down,
    out_w,
    local_sem,
    chunk_send,
    chunk_recv,
    conv_send,
    conv_recv,
):
    tokens, width = moe_hbm.shape
    e = lax.axis_index("ep")
    t = lax.axis_index("tp")
    core = lax.rem(t, 2)
    row = t // 2
    core_peer = row * 2 + (1 - core)
    y_peer = (1 - row) * 2 + core
    diagonal = (1 - row) * 2 + (1 - core)
    place = e * 4 + t
    after = lax.rem(place + 1, n * 4)
    ahead = lax.rem(place + n * 4 - 1, n * 4)
    halo_rows = halo.shape[0]
    half = n // 2
    side = e // half
    deep = lax.rem(e, half) // 2
    across = lax.rem(e, 2)
    outer = side * deep + (1 - side) * (1 - deep)
    conv_cut = tokens // CONV_PARTS

    fetches = [
        pltpu.make_async_copy(src, dst, local_sem.at[i])
        for i, (src, dst) in enumerate(
            (
                (moe_hbm, moe_in),
                (conv_hbm, conv_in),
                (taps_hbm, taps),
                (gate_hbm.at[0], gate_w),
                (up_hbm.at[0], up_w),
                (down_hbm.at[0], down_w),
                (sh_gate_hbm, sh_gate),
                (sh_up_hbm, sh_up),
                (sh_down_hbm, sh_down),
                (out_w_hbm, out_w),
            )
        )
    ]
    for fetch in fetches:
        fetch.start()

    barrier = pltpu.get_barrier_semaphore()
    greeted = [(lax.rem(e + k, n), t) for k in range(1, n)]
    greeted += [(e, core_peer), (e, y_peer)]
    greeted += [(after // 4, lax.rem(after, 4)), (ahead // 4, lax.rem(ahead, 4))]
    for device in greeted:
        pl.semaphore_signal(barrier, inc=1, device_id=device, device_id_type=MESH)

    def flip(a, b):
        return a + b - 2 * a * b

    def near_rank(j):
        return side * half + 2 * flip(deep, j // 2) + flip(across, lax.rem(j, 2))

    def far_rank(there, j):
        return (1 - side) * half + 2 * there + flip(across, j)

    def near_item(j):
        return 0 if j == 0 else j + 1

    def is_far(k):
        return (k == 1) | (k > half)

    def far_parts(k):
        v = (k // (half + 1)) * (k - half)
        q = (v + 1) // 2
        from_outer = (1 - outer) * (v // 2) + outer * (1 - q * (2 - q))
        return from_outer, (1 - outer) * lax.rem(v, 2) + outer * (v // 2)

    def packed(order):
        return sum(item * n**place for place, item in enumerate(order))

    item_order = (1 - outer) * packed((0, 1, 5, 2, 3, 4, 6, 7)) + outer * packed(
        (0, 1, 2, 5, 3, 6, 4, 7)
    )

    def remote(src, dst, kind, k, device, k_there=None):
        return pltpu.make_async_remote_copy(
            src_ref=src,
            dst_ref=dst,
            send_sem=chunk_send.at[kind, k],
            recv_sem=chunk_recv.at[kind, k if k_there is None else k_there],
            device_id=device,
            device_id_type=MESH,
        )

    def conv_copy(src, dst, kind, device):
        return pltpu.make_async_remote_copy(
            src_ref=src,
            dst_ref=dst,
            send_sem=conv_send.at[kind],
            recv_sem=conv_recv.at[kind],
            device_id=device,
            device_id_type=MESH,
        )

    def send_near(j):
        k = near_item(j)
        return remote(own.at[j], gath.at[k, t], 0, j, (near_rank(j), t), k)

    def send_near_peer(j):
        k = near_item(j)
        return remote(own_peer.at[j], gath.at[k, y_peer], 1, k, (near_rank(j), t))

    def send_far(to_outer, j):
        there = (1 - side) * to_outer + side * (1 - to_outer)
        if to_outer:
            v = (1 - outer) * (1 + j) + outer * 3 * j
        else:
            v = 2 * outer + j
        k = 1 + v + 3 * ((v + 2) // 3)
        s = half + 2 * there + j
        return remote(own.at[s], gath.at[k, t], 0, s, (far_rank(there, j), t), k)

    def arrive(k):
        return remote(own.at[k], gath.at[k, t], 0, k, (e, core_peer))

    def share_core(k, q):
        return remote(gath.at[k, q], gath.at[k, q], 2, k, (e, core_peer))

    def share_y(k, q):
        return remote(gath.at[k, q], gath.at[k, q], 1, k, (e, y_peer))

    def forward_core(k, q):
        return remote(gath.at[k, q], gath.at[k, q], 3, k, (e, core_peer))

    def reduce_core(k, q, which):
        return remote(part.at[k, q], from_core.at[which, k], 4 + which, k, (e, core_peer))

    def reduce_y(k):
        return remote(pair_sum.at[k], from_y.at[k], 6, k, (e, y_peer))

    def return_near(k):
        j = k - 1
        return remote(result.at[k], returned.at[j], 7, k, (near_rank(j), t), j)

    def return_near_peer(k):
        j = k - 1
        return remote(result_peer.at[k], returned_peer.at[j], 8, k, (near_rank(j), t), j)

    def return_far(k):
        m, j = far_parts(k)
        there = m * (1 - side) + (1 - m) * side
        s = half + 2 * deep + j
        return remote(result.at[k], returned.at[s], 7, k, (far_rank(there, j), t), s)

    normal_y = conv_copy(normal, normal_peer, 1, (e, y_peer))
    weight_y = conv_copy(weight_ref, weight_peer, 2, (e, y_peer))
    halo_copy = conv_copy(
        conv_in.at[pl.ds(tokens - halo_rows, halo_rows)],
        halo,
        0,
        (after // 4, lax.rem(after, 4)),
    )
    conv_core = conv_copy(conv_all.at[t], conv_all.at[t], 3, (e, core_peer))
    conv_pass = conv_copy(conv_all.at[y_peer], conv_all.at[y_peer], 4, (e, core_peer))
    near_y = conv_copy(near_send, near_recv, 5, (e, y_peer))

    def conv_y(q, p):
        block = conv_all.at[q, pl.ds(p * conv_cut, conv_cut)]
        return conv_copy(block, block, 6 + p, (e, y_peer))

    def column(row_data):
        return jnp.broadcast_to(row_data, (LANES, tokens)).T[:, 0:1]

    slot_rank = [near_rank(j) for j in range(half)]
    slot_rank += [far_rank(s // 2, s % 2) for s in range(half)]
    earlier = (
        lax.broadcasted_iota(jnp.int32, (tokens, tokens), 0)
        > lax.broadcasted_iota(jnp.int32, (tokens, tokens), 1)
    ).astype(jnp.float32).astype(jnp.bfloat16)
    lane = lax.broadcasted_iota(jnp.int32, (tokens, LANES), 1).astype(jnp.float32)

    def slots_of(block):
        chosen = index_ref[:, pl.ds(pl.multiple_of(block * tokens, tokens), tokens)]
        order = jnp.zeros(chosen.shape, jnp.float32)
        for s in range(1, n):
            order = order + jnp.where(chosen == slot_rank[s], float(s), 0.0)
        first, second = column(order[0:1, :]), column(order[1:2, :])
        hot_first = (lane == first).astype(jnp.float32)
        hot_second = (lane == second).astype(jnp.float32)
        before = jnp.dot(
            earlier,
            (hot_first + hot_second).astype(jnp.bfloat16),
            preferred_element_type=jnp.float32,
        )
        return (
            first * slots + jnp.sum(before * hot_first, axis=1, keepdims=True),
            second * slots + jnp.sum(before * hot_second, axis=1, keepdims=True),
        )

    def spread_of(pair, base, count):
        row_first = jnp.broadcast_to(pair[0], (tokens, LANES)).T[0:1, :]
        row_second = jnp.broadcast_to(pair[1], (tokens, LANES)).T[0:1, :]
        slot_row = base * slots + lax.broadcasted_iota(jnp.int32, (count * slots, tokens), 0)
        slot_row = slot_row.astype(jnp.float32)
        return (
            jnp.where(slot_row == row_first, 1.0, 0.0) + jnp.where(slot_row == row_second, 1.0, 0.0)
        ).astype(jnp.bfloat16)

    def share_of(pair, weights, base, count):
        slot_lane = base * slots + lax.broadcasted_iota(
            jnp.int32, (tokens, count * slots), 1
        ).astype(jnp.float32)
        share = jnp.where(slot_lane == pair[0], column(weights[0:1, :]), 0.0) + jnp.where(
            slot_lane == pair[1], column(weights[1:2, :]), 0.0
        )
        high = share.astype(jnp.bfloat16)
        return high, (share - high.astype(jnp.float32)).astype(jnp.bfloat16)

    def weighed(shares, rows):
        return jnp.dot(shares[0], rows, preferred_element_type=jnp.float32) + jnp.dot(
            shares[1], rows, preferred_element_type=jnp.float32
        )

    pair = slots_of(t)
    head = (1 - outer) * half
    spread_head = spread_of(pair, head, half)
    spread_tail = spread_of(pair, half - head, half)
    fetches[0].wait()

    def normal_rows(i, carry):
        rows = pl.ds(pl.multiple_of(i * ROW_TILE, ROW_TILE), ROW_TILE)
        normal[rows, :] = layer_scale(moe_in[rows, :], moe_gain[...]).astype(jnp.bfloat16)
        return carry

    lax.fori_loop(0, tokens // ROW_TILE, normal_rows, 0, unroll=4)

    pl.semaphore_wait(barrier, len(greeted))
    fetches[1].wait()

    @pl.when(place < n * 4 - 1)
    def _():
        halo_copy.start()

    normal_y.start()
    weight_y.start()

    def fill_own(spread, first):
        for c in range(0, width, COLS):
            rows = jnp.dot(spread, normal[:, c : c + COLS], preferred_element_type=jnp.float32)
            rows = rows.astype(jnp.bfloat16).reshape(half, slots, COLS)
            own[pl.ds(first, half), :, c : c + COLS] = rows

    fill_own(spread_head, head)
    @pl.when(outer == 0)
    def _():
        send_far(0, 0).start()
        send_far(0, 1).start()

    @pl.when(outer == 1)
    def _():
        for j in (2, 3, 1):
            send_near(j).start()

    fill_own(spread_tail, half - head)
    @pl.when(outer == 0)
    def _():
        for j in (2, 3, 1):
            send_near(j).start()

    @pl.when(outer == 1)
    def _():
        send_far(1, 0).start()

    gath[0, t] = own[0]
    share_core(0, t).start()

    fetches[2].wait()

    @pl.when(place > 0)
    def _():
        conv_copy(halo, halo, 0, (e, core_peer)).wait_recv()

    @pl.when(place > 0)
    def _():
        pad[0:halo_rows, :] = halo[...].astype(jnp.float32)

    @pl.when(place == 0)
    def _():
        pad[0:halo_rows, :] = jnp.zeros((halo_rows, width), jnp.float32)

    pad[halo_rows:, :] = conv_in[...].astype(jnp.float32)

    def strip(c, carry):
        cols = pl.ds(pl.multiple_of(c * LANES, LANES), LANES)
        running = jnp.zeros((tokens, LANES), jnp.float32)
        for k in range(reach + 1):
            start = halo_rows - reach + k
            running = running + pad[pl.ds(start, tokens), cols] * taps[pl.ds(k, 1), cols]
        mixed[:, cols] = running
        return carry

    lax.fori_loop(0, width // LANES, strip, 0)

    def conv_rows(i, carry):
        rows = pl.ds(pl.multiple_of(i * ROW_TILE, ROW_TILE), ROW_TILE)
        conv_all[t, rows, :] = jax.nn.silu(layer_scale(mixed[rows, :], conv_gain[...])).astype(
            jnp.bfloat16
        )
        return carry

    lax.fori_loop(0, tokens // ROW_TILE, conv_rows, 0, unroll=4)
    conv_core.start()

    def relay(k):
        arrive(k).wait_recv()

        @pl.when(is_far(k))
        def _():
            share_y(k, t).start()

        share_core(k, t).start()

    @pl.when(outer == 0)
    def _():
        send_far(1, 0).start()
        relay(1)

    @pl.when(outer == 1)
    def _():
        for p in range(CONV_PARTS // 2):
            conv_y(t, p).start()

    normal_y.wait_recv()
    pair_peer = slots_of(y_peer)
    spread_peer = spread_of(pair_peer, 0, half)
    for c in range(0, width, COLS):
        rows = jnp.dot(spread_peer, normal_peer[:, c : c + COLS], preferred_element_type=jnp.float32)
        rows = rows.astype(jnp.bfloat16).reshape(half, slots, COLS)
        own_peer[:, :, c : c + COLS] = rows
        gath[0, y_peer, :, c : c + COLS] = rows[0]
    @pl.when(outer == 1)
    def _():
        send_far(1, 1).start()

    for j in (2, 3, 1):
        send_near_peer(j).start()

    @pl.when(outer == 0)
    def _():
        send_far(1, 1).start()

    @pl.when(outer == 1)
    def _():
        send_far(0, 0).start()
        send_far(0, 1).start()

    forward_core(0, y_peer).start()
    relay(2)
    relay(3)
    relay(4)
    for fetch in fetches[3:6]:
        fetch.wait()

    def meet_core(k):
        reduce_core(k, core_peer, 0).wait_recv()
        reduce_core(k, core_peer, 1).wait_recv()

        @pl.when(is_far(k))
        def _():
            pair_sum[k] = (
                part[k, y_peer].astype(jnp.float32) + from_core[1, k].astype(jnp.float32)
            ).astype(jnp.bfloat16)
            reduce_y(k).start()

        @pl.when((k > 1) & (k <= half))
        def _():
            result_peer[k] = (
                part[k, y_peer].astype(jnp.float32) + from_core[1, k].astype(jnp.float32)
            ).astype(jnp.bfloat16)
            return_near_peer(k).start()
            result[k] = (
                part[k, t].astype(jnp.float32) + from_core[0, k].astype(jnp.float32)
            ).astype(jnp.bfloat16)
            return_near(k).start()

        @pl.when(k == 0)
        def _():
            returned[0] = (
                part[0, t].astype(jnp.float32) + from_core[0, 0].astype(jnp.float32)
            ).astype(jnp.bfloat16)
            returned_peer[0] = (
                part[0, y_peer].astype(jnp.float32) + from_core[1, 0].astype(jnp.float32)
            ).astype(jnp.bfloat16)

    def meet_y(k):
        reduce_y(k).wait_recv()
        summed = part[k, t].astype(jnp.float32) + from_core[0, k].astype(jnp.float32)
        result[k] = (summed + from_y[k].astype(jnp.float32)).astype(jnp.bfloat16)
        return_far(k).start()

    def step(i, carry):
        k = lax.rem(carry, n)
        later = lax.rem(carry // n, n)
        share_core(k, core_peer).wait_recv()
        forward_core(k, diagonal).wait_recv()
        rows = gath[k].reshape(4 * slots, width)
        hidden = gated(rows, gate_w[...], up_w[...])
        for c in range(0, width, COLS):
            piece = jnp.dot(hidden, down_w[:, c : c + COLS], preferred_element_type=jnp.float32)
            part[k, :, :, c : c + COLS] = piece.astype(jnp.bfloat16).reshape(4, slots, COLS)
        reduce_core(k, diagonal, 1).start()
        reduce_core(k, core_peer, 0).start()

        @pl.when((i == 0) & (outer == 1))
        def _():
            relay(1)
            conv_y(t, 2).start()

        @pl.when(i == outer)
        def _():
            relay(5)

        @pl.when((i == 0) & (outer == 0))
        def _():
            for p in range(CONV_PARTS // 2):
                conv_y(t, p).start()

        @pl.when((i == 2) & (outer == 1))
        def _():
            relay(6)
            relay(7)

        @pl.when((i == 7) & (outer == 1))
        def _():
            meet_y(5)

        meet_first = (i == n - 1) | ((outer == 0) & (i >= 4)) | ((outer == 1) & (lax.rem(i, 2) == 0) & (i < 6))

        @pl.when(meet_first)
        def _():
            meet_core(k)

        @pl.when((i == 4) & (outer == 0))
        def _():
            meet_y(1)
            relay(6)

        @pl.when((i == 5) & (outer == 0))
        def _():
            meet_y(5)
            relay(7)

        @pl.when(i + 1 < n)
        def _():
            share_y(later, y_peer).wait_recv()
            forward_core(later, y_peer).start()

        @pl.when(jnp.logical_not(meet_first))
        def _():
            meet_core(k)

        @pl.when((i == 3) & (outer == 1))
        def _():
            meet_y(1)

        return carry // n

    lax.fori_loop(0, n, step, item_order)

    @pl.when(outer == 0)
    def _():
        conv_y(t, 2).start()

    conv_y(t, 3).start()

    meet_y(6)

    meet_y(7)
    for j in (1, 2, 3):
        remote(result.at[j], returned_peer.at[j], 8, j, (e, core_peer)).wait_recv()
    weight_y.wait_recv()
    peer_share = share_of(pair_peer, weight_peer, 0, half)
    for c in range(0, width, COLS):
        rows = returned_peer[:, :, c : c + COLS].reshape(half * slots, COLS)
        near_send[:, c : c + COLS] = weighed(peer_share, rows).astype(jnp.bfloat16)
    near_y.start()


    for p in range(CONV_PARTS):
        conv_y(y_peer, p).wait_recv()
    conv_pass.start()

    for fetch in fetches[6:]:
        fetch.wait()
    conv_copy(conv_all.at[core_peer], conv_all.at[core_peer], 3, (e, core_peer)).wait_recv()
    conv_copy(conv_all.at[diagonal], conv_all.at[diagonal], 4, (e, core_peer)).wait_recv()

    for q in range(4):
        conv_out[q * tokens : (q + 1) * tokens, :] = jnp.dot(
            conv_all[q], out_w[...], preferred_element_type=jnp.float32
        ).astype(jnp.bfloat16)

    shared = gated(normal[...], sh_gate[...], sh_up[...])
    near_share = share_of(pair, weight_ref, 0, half)
    for j in (1, 2, 3):
        remote(result.at[j], returned.at[j], 7, j, (e, core_peer)).wait_recv()
    for c in range(0, width, COLS):
        rows = returned[0:half, :, c : c + COLS].reshape(half * slots, COLS)
        piece = jnp.dot(shared, sh_down[:, c : c + COLS], preferred_element_type=jnp.float32)
        total[:, c : c + COLS] = piece + weighed(near_share, rows)

    far_share = share_of(pair, weight_ref, half, half)
    near_y.wait_recv()
    for s in range(half, n):
        remote(result.at[s], returned.at[s], 7, s, (e, core_peer)).wait_recv()
    for c in range(0, width, COLS):
        rows = returned[half:n, :, c : c + COLS].reshape(half * slots, COLS)
        piece = total[:, c : c + COLS] + near_recv[:, c : c + COLS].astype(jnp.float32)
        moe_out[:, c : c + COLS] = (piece + weighed(far_share, rows)).astype(jnp.bfloat16)

    @pl.when(place < n * 4 - 1)
    def _():
        halo_copy.wait_send()

    for copy in (normal_y, weight_y, conv_core, conv_pass, near_y):
        copy.wait_send()
    for p in range(CONV_PARTS):
        conv_y(t, p).wait_send()

    def drain(k, carry):
        @pl.when(k > 0)
        def _():
            arrive(k).wait_send()

        @pl.when(is_far(k))
        def _():
            share_y(k, t).wait_send()
            reduce_y(k).wait_send()

        @pl.when((k > 1) & (k <= half))
        def _():
            share_y(k, t).wait_send()
            return_near_peer(k).wait_send()

        @pl.when(k > 0)
        def _():
            remote(result.at[k], returned.at[k], 7, k, (e, core_peer)).wait_send()

        share_core(k, t).wait_send()
        forward_core(k, y_peer).wait_send()
        reduce_core(k, diagonal, 1).wait_send()
        reduce_core(k, core_peer, 0).wait_send()
        return carry

    lax.fori_loop(0, n, drain, 0)


def fused(
    conv_input,
    conv_kernel,
    conv_gain,
    out_weight,
    moe_input,
    moe_gain,
    expert_gate,
    expert_up,
    expert_down,
    shared_gate,
    shared_up,
    shared_down,
    expert_index,
    routing_weight,
):
    n = lax.axis_size("ep")
    parts = lax.axis_size("tp")
    tokens, width = moe_input.shape
    slots = 3 * tokens * routing_weight.shape[1] // (2 * n)
    hidden = expert_gate.shape[2]
    shared_hidden = shared_gate.shape[1]
    reach = conv_kernel.shape[0] - 1
    halo_rows = -(-reach // ROW_TILE) * ROW_TILE
    out_cols = out_weight.shape[1]
    bf16 = jnp.bfloat16
    chunk = (n, slots, width)
    half_chunk = (n // 2, slots, width)
    rows = (tokens, width)
    vmem = pl.BlockSpec(memory_space=pltpu.VMEM)
    hbm = pl.BlockSpec(memory_space=pl.ANY)
    return pl.pallas_call(
        functools.partial(fused_kernel, n, slots, reach),
        out_shape=(
            pltpu.VMEM((parts * tokens, out_cols), bf16),
            pltpu.VMEM(rows, bf16),
        ),
        in_specs=[hbm, hbm, vmem, hbm, hbm, vmem, hbm, hbm, hbm, hbm, hbm, hbm, vmem, vmem],
        out_specs=(vmem, vmem),
        scratch_shapes=[
            pltpu.VMEM(chunk, bf16),
            pltpu.VMEM(half_chunk, bf16),
            pltpu.VMEM((n, parts, slots, width), bf16),
            pltpu.VMEM((n, parts, slots, width), bf16),
            pltpu.VMEM((2,) + chunk, bf16),
            pltpu.VMEM(chunk, bf16),
            pltpu.VMEM(chunk, bf16),
            pltpu.VMEM(chunk, bf16),
            pltpu.VMEM(chunk, bf16),
            pltpu.VMEM(chunk, bf16),
            pltpu.VMEM(half_chunk, bf16),
            pltpu.VMEM(rows, bf16),
            pltpu.VMEM(rows, bf16),
            pltpu.VMEM((2, tokens), jnp.float32),
            pltpu.VMEM(rows, bf16),
            pltpu.VMEM(rows, bf16),
            pltpu.VMEM(rows, jnp.float32),
            pltpu.VMEM((halo_rows, width), bf16),
            pltpu.VMEM((halo_rows + tokens, width), jnp.float32),
            pltpu.VMEM(rows, jnp.float32),
            pltpu.VMEM((parts, tokens, width), bf16),
            pltpu.VMEM(rows, bf16),
            pltpu.VMEM((reach + 1, width), jnp.float32),
            pltpu.VMEM(rows, bf16),
            pltpu.VMEM((width, hidden), bf16),
            pltpu.VMEM((width, hidden), bf16),
            pltpu.VMEM((hidden, width), bf16),
            pltpu.VMEM((width, shared_hidden), bf16),
            pltpu.VMEM((width, shared_hidden), bf16),
            pltpu.VMEM((shared_hidden, width), bf16),
            pltpu.VMEM((width, out_cols), bf16),
            pltpu.SemaphoreType.DMA((10,)),
            pltpu.SemaphoreType.DMA((9, n)),
            pltpu.SemaphoreType.DMA((9, n)),
            pltpu.SemaphoreType.DMA((6 + CONV_PARTS,)),
            pltpu.SemaphoreType.DMA((6 + CONV_PARTS,)),
        ],
        compiler_params=pltpu.CompilerParams(
            collective_id=0, has_side_effects=True, vmem_limit_bytes=60 * 1024 * 1024
        ),
    )(
        conv_input,
        conv_kernel,
        conv_gain.reshape(1, width),
        out_weight,
        moe_input,
        moe_gain.reshape(1, width),
        expert_gate,
        expert_up,
        expert_down,
        shared_gate,
        shared_up,
        shared_down,
        expert_index.T,
        routing_weight.T,
    )


def fits_fused(args):
    n, parts = lax.axis_size("ep"), lax.axis_size("tp")
    conv_input, conv_kernel, moe_input = args[0], args[1], args[4]
    top_count = args[13].shape[1]
    tokens, width = moe_input.shape
    slots = 3 * tokens * top_count // (2 * n)
    return (
        parts == 4
        and top_count == 2
        and args[6].shape[0] == 1
        and conv_input.shape == moe_input.shape
        and conv_kernel.shape[0] - 1 <= tokens
        and tokens % LANES == 0
        and width % COLS == 0
        and slots % ROW_TILE == 0
        and slots >= ROW_TILE
        and n == 8
    )


def either(*args):
    return fused(*args) if fits_fused(args) else on_device(*args)


def solution(mesh):
    in_specs = (
        P(("ep", "tp"), None),
        P(),
        P(),
        P(None, "tp"),
        P(("ep", "tp"), None),
        P(),
        P("ep", None, "tp"),
        P("ep", None, "tp"),
        P("ep", "tp", None),
        P(),
        P(),
        P(),
        P("ep", None),
        P(("ep", "tp"), None),
    )
    out_specs = (P("ep", "tp"), P(("ep", "tp"), None))
    return jax.shard_map(
        either, mesh=mesh, in_specs=in_specs, out_specs=out_specs, check_vma=False
    )
```

```python
import functools

import jax
import jax.numpy as jnp
from jax import lax
from jax.experimental import pallas as pl
from jax.experimental.pallas import tpu as pltpu
from jax.sharding import PartitionSpec as P

NORM_EPS = 1e-05


def passed_along(block, axis, distance):
    devices = range(lax.axis_size(axis))
    route = [(i - distance, i) for i in devices if i - distance in devices]
    return lax.ppermute(block, axis, route)


def layer_scale(row_data, gain_vec):
    values = row_data.astype(jnp.float32)
    center = values - jnp.mean(values, axis=-1, keepdims=True)
    spread = jnp.mean(center * center, axis=-1, keepdims=True)
    return center * lax.rsqrt(spread + NORM_EPS) * gain_vec


def depthwise(padded, kernel, length):
    running = jnp.zeros((length, padded.shape[1]), jnp.float32)
    for offset in range(kernel.shape[0]):
        running = running + padded[offset : offset + length].astype(jnp.float32) * kernel[offset]
    return running


def slot_table(block_index, experts, slot_count):
    onehot = (
        block_index[:, :, None] == jnp.arange(experts, dtype=jnp.int32)[None, None, :]
    ).astype(jnp.int32)
    before = jnp.cumsum(onehot, axis=1) - onehot
    position = jnp.sum(before * onehot, axis=2)
    return block_index * slot_count + position


def fill_slots(row_data, entry_slot, top_count, total_slots):
    block_count = entry_slot.shape[0]
    entries = entry_slot.shape[1]
    block_ids = jnp.arange(block_count, dtype=jnp.int32)[:, None]
    source = jnp.arange(entries, dtype=jnp.int32)[None, :] // top_count
    slot_row = (
        jnp.zeros((block_count, total_slots), jnp.int32).at[block_ids, entry_slot].set(source)
    )
    filled = jnp.zeros((block_count, total_slots), jnp.int32).at[block_ids, entry_slot].set(1)
    picked = row_data[block_ids, slot_row]
    return jnp.where(filled[:, :, None] > 0, picked, jnp.zeros((), row_data.dtype))


def gated(row_data, gate_weight, up_weight):
    gate_proj = jnp.dot(row_data, gate_weight, preferred_element_type=jnp.float32)
    up_proj = jnp.dot(row_data, up_weight, preferred_element_type=jnp.float32)
    return (jax.nn.silu(gate_proj) * up_proj).astype(jnp.bfloat16)


def on_device(
    conv_input,
    conv_kernel,
    conv_gain,
    out_weight,
    moe_input,
    moe_gain,
    expert_gate,
    expert_up,
    expert_down,
    shared_gate,
    shared_up,
    shared_down,
    expert_index,
    routing_weight,
):
    reach = conv_kernel.shape[0] - 1
    length = conv_input.shape[0]
    halo_rows = passed_along(conv_input[length - reach :], ("ep", "tp"), 1)
    padded = jnp.concatenate([halo_rows, conv_input], axis=0)
    mixed_rows = depthwise(padded, conv_kernel, length)
    normed = jax.nn.silu(layer_scale(mixed_rows, conv_gain)).astype(jnp.bfloat16)
    conv_out = jnp.dot(
        lax.all_gather(normed, "tp", axis=0, tiled=True),
        out_weight,
        preferred_element_type=jnp.float32,
    ).astype(jnp.bfloat16)
    tp_parts = lax.axis_size("tp")
    tp_index = lax.axis_index("tp")
    ep_ranks = lax.axis_size("ep")
    tok_count = moe_input.shape[0]
    top_count = routing_weight.shape[1]
    model_width = moe_input.shape[1]
    experts = ep_ranks * expert_gate.shape[0]
    slot_count = 3 * tok_count * top_count // (2 * experts)
    total_slots = experts * slot_count
    normal = layer_scale(moe_input, moe_gain).astype(jnp.bfloat16)
    group_slots = slot_table(
        expert_index.reshape(tp_parts, tok_count * top_count), experts, slot_count
    )
    own_slots = lax.dynamic_index_in_dim(group_slots, tp_index, 0, keepdims=True)
    gate_local = expert_gate[0]
    up_local = expert_up[0]
    down_local = expert_down[0]
    own_rows = fill_slots(normal[None], own_slots, top_count, total_slots)
    own_rows = own_rows.reshape(ep_ranks, slot_count, model_width)
    arrived = lax.all_to_all(own_rows, "ep", split_axis=0, concat_axis=0, tiled=True)
    hidden = gated(
        lax.all_gather(
            arrived.reshape(ep_ranks * slot_count, model_width), "tp", axis=0, tiled=True
        ),
        gate_local,
        up_local,
    )
    summed = lax.psum_scatter(
        jnp.dot(hidden, down_local, preferred_element_type=jnp.float32).astype(jnp.bfloat16),
        "tp",
        scatter_dimension=0,
        tiled=True,
    )
    returned = lax.all_to_all(
        summed.reshape(ep_ranks, slot_count, model_width),
        "ep",
        split_axis=0,
        concat_axis=0,
        tiled=True,
    )
    picked = returned.reshape(total_slots, model_width)[own_slots[0]]
    picked = picked.reshape(tok_count, top_count, model_width).astype(jnp.float32)
    routed = jnp.sum(picked * routing_weight[:, :, None], axis=1)
    shared_hidden = gated(normal, shared_gate, shared_up)
    shared_part = jnp.dot(shared_hidden, shared_down, preferred_element_type=jnp.float32)
    moe_out = (shared_part + routed).astype(jnp.bfloat16)
    return (conv_out, moe_out)


LANES = 128
ROW_TILE = 16
COLS = 512
CONV_PARTS = 4
MESH = pl.DeviceIdType.MESH


def fused_kernel(
    n,
    slots,
    reach,
    conv_hbm,
    taps_hbm,
    conv_gain,
    out_w_hbm,
    moe_hbm,
    moe_gain,
    gate_hbm,
    up_hbm,
    down_hbm,
    sh_gate_hbm,
    sh_up_hbm,
    sh_down_hbm,
    index_ref,
    weight_ref,
    conv_out,
    moe_out,
    own,
    own_peer,
    gath,
    part,
    from_core,
    pair_sum,
    from_y,
    result,
    result_peer,
    returned,
    returned_peer,
    normal,
    normal_peer,
    weight_peer,
    near_send,
    near_recv,
    total,
    halo,
    pad,
    mixed,
    conv_all,
    conv_in,
    taps,
    moe_in,
    gate_w,
    up_w,
    down_w,
    sh_gate,
    sh_up,
    sh_down,
    out_w,
    local_sem,
    chunk_send,
    chunk_recv,
    conv_send,
    conv_recv,
):
    tokens, width = moe_hbm.shape
    e = lax.axis_index("ep")
    t = lax.axis_index("tp")
    core = lax.rem(t, 2)
    row = t // 2
    core_peer = row * 2 + (1 - core)
    y_peer = (1 - row) * 2 + core
    diagonal = (1 - row) * 2 + (1 - core)
    place = e * 4 + t
    after = lax.rem(place + 1, n * 4)
    ahead = lax.rem(place + n * 4 - 1, n * 4)
    halo_rows = halo.shape[0]
    half = n // 2
    side = e // half
    deep = lax.rem(e, half) // 2
    across = lax.rem(e, 2)
    outer = side * deep + (1 - side) * (1 - deep)
    conv_cut = tokens // CONV_PARTS

    fetches = [
        pltpu.make_async_copy(src, dst, local_sem.at[i])
        for i, (src, dst) in enumerate(
            (
                (moe_hbm, moe_in),
                (conv_hbm, conv_in),
                (taps_hbm, taps),
                (gate_hbm.at[0], gate_w),
                (up_hbm.at[0], up_w),
                (down_hbm.at[0], down_w),
                (sh_gate_hbm, sh_gate),
                (sh_up_hbm, sh_up),
                (sh_down_hbm, sh_down),
                (out_w_hbm, out_w),
            )
        )
    ]
    for fetch in fetches:
        fetch.start()

    barrier = pltpu.get_barrier_semaphore()
    greeted = [(lax.rem(e + k, n), t) for k in range(1, n)]
    greeted += [(e, core_peer), (e, y_peer)]
    greeted += [(after // 4, lax.rem(after, 4)), (ahead // 4, lax.rem(ahead, 4))]
    for device in greeted:
        pl.semaphore_signal(barrier, inc=1, device_id=device, device_id_type=MESH)

    def flip(a, b):
        return a + b - 2 * a * b

    def near_rank(j):
        return side * half + 2 * flip(deep, j // 2) + flip(across, lax.rem(j, 2))

    def far_rank(there, j):
        return (1 - side) * half + 2 * there + flip(across, j)

    def near_item(j):
        return 0 if j == 0 else j + 1

    def is_far(k):
        return (k == 1) | (k > half)

    def far_parts(k):
        v = (k // (half + 1)) * (k - half)
        q = (v + 1) // 2
        from_outer = (1 - outer) * (v // 2) + outer * (1 - q * (2 - q))
        return from_outer, (1 - outer) * lax.rem(v, 2) + outer * (v // 2)

    def packed(order):
        return sum(item * n**place for place, item in enumerate(order))

    item_order = (1 - outer) * packed((0, 1, 5, 2, 3, 4, 6, 7)) + outer * packed(
        (0, 1, 2, 5, 3, 6, 4, 7)
    )

    def remote(src, dst, kind, k, device, k_there=None):
        return pltpu.make_async_remote_copy(
            src_ref=src,
            dst_ref=dst,
            send_sem=chunk_send.at[kind, k],
            recv_sem=chunk_recv.at[kind, k if k_there is None else k_there],
            device_id=device,
            device_id_type=MESH,
        )

    def conv_copy(src, dst, kind, device):
        return pltpu.make_async_remote_copy(
            src_ref=src,
            dst_ref=dst,
            send_sem=conv_send.at[kind],
            recv_sem=conv_recv.at[kind],
            device_id=device,
            device_id_type=MESH,
        )

    def send_near(j):
        k = near_item(j)
        return remote(own.at[j], gath.at[k, t], 0, j, (near_rank(j), t), k)

    def send_near_peer(j):
        k = near_item(j)
        return remote(own_peer.at[j], gath.at[k, y_peer], 1, k, (near_rank(j), t))

    def send_far(to_outer, j):
        there = (1 - side) * to_outer + side * (1 - to_outer)
        if to_outer:
            v = (1 - outer) * (1 + j) + outer * 3 * j
        else:
            v = 2 * outer + j
        k = 1 + v + 3 * ((v + 2) // 3)
        s = half + 2 * there + j
        return remote(own.at[s], gath.at[k, t], 0, s, (far_rank(there, j), t), k)

    def arrive(k):
        return remote(own.at[k], gath.at[k, t], 0, k, (e, core_peer))

    def share_core(k, q):
        return remote(gath.at[k, q], gath.at[k, q], 2, k, (e, core_peer))

    def share_y(k, q):
        return remote(gath.at[k, q], gath.at[k, q], 1, k, (e, y_peer))

    def forward_core(k, q):
        return remote(gath.at[k, q], gath.at[k, q], 3, k, (e, core_peer))

    def reduce_core(k, q, which):
        return remote(part.at[k, q], from_core.at[which, k], 4 + which, k, (e, core_peer))

    def reduce_y(k):
        return remote(pair_sum.at[k], from_y.at[k], 6, k, (e, y_peer))

    def return_near(k):
        j = k - 1
        return remote(result.at[k], returned.at[j], 7, k, (near_rank(j), t), j)

    def return_near_peer(k):
        j = k - 1
        return remote(result_peer.at[k], returned_peer.at[j], 8, k, (near_rank(j), t), j)

    def return_far(k):
        m, j = far_parts(k)
        there = m * (1 - side) + (1 - m) * side
        s = half + 2 * deep + j
        return remote(result.at[k], returned.at[s], 7, k, (far_rank(there, j), t), s)

    normal_y = conv_copy(normal, normal_peer, 1, (e, y_peer))
    weight_y = conv_copy(weight_ref, weight_peer, 2, (e, y_peer))
    halo_copy = conv_copy(
        conv_in.at[pl.ds(tokens - halo_rows, halo_rows)],
        halo,
        0,
        (after // 4, lax.rem(after, 4)),
    )
    conv_core = conv_copy(conv_all.at[t], conv_all.at[t], 3, (e, core_peer))
    conv_pass = conv_copy(conv_all.at[y_peer], conv_all.at[y_peer], 4, (e, core_peer))
    near_y = conv_copy(near_send, near_recv, 5, (e, y_peer))

    def conv_y(q, p):
        block = conv_all.at[q, pl.ds(p * conv_cut, conv_cut)]
        return conv_copy(block, block, 6 + p, (e, y_peer))

    def column(row_data):
        return jnp.broadcast_to(row_data, (LANES, tokens)).T[:, 0:1]

    slot_rank = [near_rank(j) for j in range(half)]
    slot_rank += [far_rank(s // 2, s % 2) for s in range(half)]
    earlier = (
        lax.broadcasted_iota(jnp.int32, (tokens, tokens), 0)
        > lax.broadcasted_iota(jnp.int32, (tokens, tokens), 1)
    ).astype(jnp.float32).astype(jnp.bfloat16)
    lane = lax.broadcasted_iota(jnp.int32, (tokens, LANES), 1).astype(jnp.float32)

    def slots_of(block):
        chosen = index_ref[:, pl.ds(pl.multiple_of(block * tokens, tokens), tokens)]
        order = jnp.zeros(chosen.shape, jnp.float32)
        for s in range(1, n):
            order = order + jnp.where(chosen == slot_rank[s], float(s), 0.0)
        first, second = column(order[0:1, :]), column(order[1:2, :])
        hot_first = (lane == first).astype(jnp.float32)
        hot_second = (lane == second).astype(jnp.float32)
        before = jnp.dot(
            earlier,
            (hot_first + hot_second).astype(jnp.bfloat16),
            preferred_element_type=jnp.float32,
        )
        return (
            first * slots + jnp.sum(before * hot_first, axis=1, keepdims=True),
            second * slots + jnp.sum(before * hot_second, axis=1, keepdims=True),
        )

    def spread_of(pair, base, count):
        row_first = jnp.broadcast_to(pair[0], (tokens, LANES)).T[0:1, :]
        row_second = jnp.broadcast_to(pair[1], (tokens, LANES)).T[0:1, :]
        slot_row = base * slots + lax.broadcasted_iota(jnp.int32, (count * slots, tokens), 0)
        slot_row = slot_row.astype(jnp.float32)
        return (
            jnp.where(slot_row == row_first, 1.0, 0.0) + jnp.where(slot_row == row_second, 1.0, 0.0)
        ).astype(jnp.bfloat16)

    def share_of(pair, weights, base, count):
        slot_lane = base * slots + lax.broadcasted_iota(
            jnp.int32, (tokens, count * slots), 1
        ).astype(jnp.float32)
        share = jnp.where(slot_lane == pair[0], column(weights[0:1, :]), 0.0) + jnp.where(
            slot_lane == pair[1], column(weights[1:2, :]), 0.0
        )
        high = share.astype(jnp.bfloat16)
        return high, (share - high.astype(jnp.float32)).astype(jnp.bfloat16)

    def weighed(shares, rows):
        return jnp.dot(shares[0], rows, preferred_element_type=jnp.float32) + jnp.dot(
            shares[1], rows, preferred_element_type=jnp.float32
        )

    pair = slots_of(t)
    head = (1 - outer) * half
    spread_head = spread_of(pair, head, half)
    spread_tail = spread_of(pair, half - head, half)
    fetches[0].wait()

    def normal_rows(i, carry):
        rows = pl.ds(pl.multiple_of(i * ROW_TILE, ROW_TILE), ROW_TILE)
        normal[rows, :] = layer_scale(moe_in[rows, :], moe_gain[...]).astype(jnp.bfloat16)
        return carry

    lax.fori_loop(0, tokens // ROW_TILE, normal_rows, 0, unroll=4)

    pl.semaphore_wait(barrier, len(greeted))
    fetches[1].wait()

    @pl.when(place < n * 4 - 1)
    def _():
        halo_copy.start()

    normal_y.start()
    weight_y.start()

    def fill_own(spread, first):
        for c in range(0, width, COLS):
            rows = jnp.dot(spread, normal[:, c : c + COLS], preferred_element_type=jnp.float32)
            rows = rows.astype(jnp.bfloat16).reshape(half, slots, COLS)
            own[pl.ds(first, half), :, c : c + COLS] = rows

    fill_own(spread_head, head)
    @pl.when(outer == 0)
    def _():
        send_far(0, 0).start()
        send_far(0, 1).start()

    @pl.when(outer == 1)
    def _():
        for j in (2, 3, 1):
            send_near(j).start()

    fill_own(spread_tail, half - head)
    @pl.when(outer == 0)
    def _():
        for j in (2, 3, 1):
            send_near(j).start()

    @pl.when(outer == 1)
    def _():
        send_far(1, 0).start()

    gath[0, t] = own[0]
    share_core(0, t).start()

    fetches[2].wait()

    @pl.when(place > 0)
    def _():
        conv_copy(halo, halo, 0, (e, core_peer)).wait_recv()

    @pl.when(place > 0)
    def _():
        pad[0:halo_rows, :] = halo[...].astype(jnp.float32)

    @pl.when(place == 0)
    def _():
        pad[0:halo_rows, :] = jnp.zeros((halo_rows, width), jnp.float32)

    pad[halo_rows:, :] = conv_in[...].astype(jnp.float32)

    def strip(c, carry):
        cols = pl.ds(pl.multiple_of(c * LANES, LANES), LANES)
        running = jnp.zeros((tokens, LANES), jnp.float32)
        for k in range(reach + 1):
            start = halo_rows - reach + k
            running = running + pad[pl.ds(start, tokens), cols] * taps[pl.ds(k, 1), cols]
        mixed[:, cols] = running
        return carry

    lax.fori_loop(0, width // LANES, strip, 0)

    def conv_rows(i, carry):
        rows = pl.ds(pl.multiple_of(i * ROW_TILE, ROW_TILE), ROW_TILE)
        conv_all[t, rows, :] = jax.nn.silu(layer_scale(mixed[rows, :], conv_gain[...])).astype(
            jnp.bfloat16
        )
        return carry

    lax.fori_loop(0, tokens // ROW_TILE, conv_rows, 0, unroll=4)
    conv_core.start()

    def relay(k):
        arrive(k).wait_recv()

        @pl.when(is_far(k))
        def _():
            share_y(k, t).start()

        share_core(k, t).start()

    @pl.when(outer == 0)
    def _():
        send_far(1, 0).start()
        relay(1)

    @pl.when(outer == 1)
    def _():
        for p in range(CONV_PARTS // 2):
            conv_y(t, p).start()

    normal_y.wait_recv()
    pair_peer = slots_of(y_peer)
    spread_peer = spread_of(pair_peer, 0, half)
    for c in range(0, width, COLS):
        rows = jnp.dot(spread_peer, normal_peer[:, c : c + COLS], preferred_element_type=jnp.float32)
        rows = rows.astype(jnp.bfloat16).reshape(half, slots, COLS)
        own_peer[:, :, c : c + COLS] = rows
        gath[0, y_peer, :, c : c + COLS] = rows[0]
    @pl.when(outer == 1)
    def _():
        send_far(1, 1).start()

    for j in (2, 3, 1):
        send_near_peer(j).start()

    @pl.when(outer == 0)
    def _():
        send_far(1, 1).start()

    @pl.when(outer == 1)
    def _():
        send_far(0, 0).start()
        send_far(0, 1).start()

    forward_core(0, y_peer).start()
    relay(2)
    relay(3)
    relay(4)
    for fetch in fetches[3:6]:
        fetch.wait()

    def meet_core(k):
        reduce_core(k, core_peer, 0).wait_recv()
        reduce_core(k, core_peer, 1).wait_recv()

        @pl.when(is_far(k))
        def _():
            pair_sum[k] = (
                part[k, y_peer].astype(jnp.float32) + from_core[1, k].astype(jnp.float32)
            ).astype(jnp.bfloat16)
            reduce_y(k).start()

        @pl.when((k > 1) & (k <= half))
        def _():
            result_peer[k] = (
                part[k, y_peer].astype(jnp.float32) + from_core[1, k].astype(jnp.float32)
            ).astype(jnp.bfloat16)
            return_near_peer(k).start()
            result[k] = (
                part[k, t].astype(jnp.float32) + from_core[0, k].astype(jnp.float32)
            ).astype(jnp.bfloat16)
            return_near(k).start()

        @pl.when(k == 0)
        def _():
            returned[0] = (
                part[0, t].astype(jnp.float32) + from_core[0, 0].astype(jnp.float32)
            ).astype(jnp.bfloat16)
            returned_peer[0] = (
                part[0, y_peer].astype(jnp.float32) + from_core[1, 0].astype(jnp.float32)
            ).astype(jnp.bfloat16)

    def meet_y(k):
        reduce_y(k).wait_recv()
        summed = part[k, t].astype(jnp.float32) + from_core[0, k].astype(jnp.float32)
        result[k] = (summed + from_y[k].astype(jnp.float32)).astype(jnp.bfloat16)
        return_far(k).start()

    def step(i, carry):
        k = lax.rem(carry, n)
        later = lax.rem(carry // n, n)
        share_core(k, core_peer).wait_recv()
        forward_core(k, diagonal).wait_recv()
        rows = gath[k].reshape(4 * slots, width)
        hidden = gated(rows, gate_w[...], up_w[...])
        for c in range(0, width, COLS):
            piece = jnp.dot(hidden, down_w[:, c : c + COLS], preferred_element_type=jnp.float32)
            part[k, :, :, c : c + COLS] = piece.astype(jnp.bfloat16).reshape(4, slots, COLS)
        reduce_core(k, diagonal, 1).start()
        reduce_core(k, core_peer, 0).start()

        @pl.when((i == 0) & (outer == 1))
        def _():
            relay(1)
            conv_y(t, 2).start()

        @pl.when(i == outer)
        def _():
            relay(5)

        @pl.when((i == 0) & (outer == 0))
        def _():
            conv_y(t, 0).start()

        @pl.when((i == 2) & (outer == 1))
        def _():
            relay(6)
            relay(7)

        @pl.when((i == 7) & (outer == 1))
        def _():
            meet_y(5)

        meet_first = (i == n - 1) | ((outer == 0) & (i >= 4)) | ((outer == 1) & (lax.rem(i, 2) == 0) & (i < 6))

        @pl.when(meet_first)
        def _():
            meet_core(k)

        @pl.when((i == 4) & (outer == 0))
        def _():
            relay(6)
            meet_y(1)

        @pl.when((i == 5) & (outer == 0))
        def _():
            meet_y(5)
            relay(7)

        @pl.when(i + 1 < n)
        def _():
            share_y(later, y_peer).wait_recv()
            forward_core(later, y_peer).start()

        @pl.when(jnp.logical_not(meet_first))
        def _():
            meet_core(k)

        @pl.when((i == 3) & (outer == 1))
        def _():
            meet_y(1)

        return carry // n

    lax.fori_loop(0, n, step, item_order)

    @pl.when(outer == 0)
    def _():
        conv_y(t, 1).start()
        conv_y(t, 2).start()

    conv_y(t, 3).start()

    meet_y(6)

    meet_y(7)
    for j in (1, 2, 3):
        remote(result.at[j], returned_peer.at[j], 8, j, (e, core_peer)).wait_recv()
    weight_y.wait_recv()
    peer_share = share_of(pair_peer, weight_peer, 0, half)
    for c in range(0, width, COLS):
        rows = returned_peer[:, :, c : c + COLS].reshape(half * slots, COLS)
        near_send[:, c : c + COLS] = weighed(peer_share, rows).astype(jnp.bfloat16)
    near_y.start()


    for p in range(CONV_PARTS):
        conv_y(y_peer, p).wait_recv()
    conv_pass.start()

    for fetch in fetches[6:]:
        fetch.wait()
    conv_copy(conv_all.at[core_peer], conv_all.at[core_peer], 3, (e, core_peer)).wait_recv()
    conv_copy(conv_all.at[diagonal], conv_all.at[diagonal], 4, (e, core_peer)).wait_recv()

    for q in range(4):
        conv_out[q * tokens : (q + 1) * tokens, :] = jnp.dot(
            conv_all[q], out_w[...], preferred_element_type=jnp.float32
        ).astype(jnp.bfloat16)

    shared = gated(normal[...], sh_gate[...], sh_up[...])
    near_share = share_of(pair, weight_ref, 0, half)
    for j in (1, 2, 3):
        remote(result.at[j], returned.at[j], 7, j, (e, core_peer)).wait_recv()
    for c in range(0, width, COLS):
        rows = returned[0:half, :, c : c + COLS].reshape(half * slots, COLS)
        piece = jnp.dot(shared, sh_down[:, c : c + COLS], preferred_element_type=jnp.float32)
        total[:, c : c + COLS] = piece + weighed(near_share, rows)

    far_share = share_of(pair, weight_ref, half, half)
    near_y.wait_recv()
    for s in range(half, n):
        remote(result.at[s], returned.at[s], 7, s, (e, core_peer)).wait_recv()
    for c in range(0, width, COLS):
        rows = returned[half:n, :, c : c + COLS].reshape(half * slots, COLS)
        piece = total[:, c : c + COLS] + near_recv[:, c : c + COLS].astype(jnp.float32)
        moe_out[:, c : c + COLS] = (piece + weighed(far_share, rows)).astype(jnp.bfloat16)

    @pl.when(place < n * 4 - 1)
    def _():
        halo_copy.wait_send()

    for copy in (normal_y, weight_y, conv_core, conv_pass, near_y):
        copy.wait_send()
    for p in range(CONV_PARTS):
        conv_y(t, p).wait_send()

    def drain(k, carry):
        @pl.when(k > 0)
        def _():
            arrive(k).wait_send()

        @pl.when(is_far(k))
        def _():
            share_y(k, t).wait_send()
            reduce_y(k).wait_send()

        @pl.when((k > 1) & (k <= half))
        def _():
            share_y(k, t).wait_send()
            return_near_peer(k).wait_send()

        @pl.when(k > 0)
        def _():
            remote(result.at[k], returned.at[k], 7, k, (e, core_peer)).wait_send()

        share_core(k, t).wait_send()
        forward_core(k, y_peer).wait_send()
        reduce_core(k, diagonal, 1).wait_send()
        reduce_core(k, core_peer, 0).wait_send()
        return carry

    lax.fori_loop(0, n, drain, 0)


def fused(
    conv_input,
    conv_kernel,
    conv_gain,
    out_weight,
    moe_input,
    moe_gain,
    expert_gate,
    expert_up,
    expert_down,
    shared_gate,
    shared_up,
    shared_down,
    expert_index,
    routing_weight,
):
    n = lax.axis_size("ep")
    parts = lax.axis_size("tp")
    tokens, width = moe_input.shape
    slots = 3 * tokens * routing_weight.shape[1] // (2 * n)
    hidden = expert_gate.shape[2]
    shared_hidden = shared_gate.shape[1]
    reach = conv_kernel.shape[0] - 1
    halo_rows = -(-reach // ROW_TILE) * ROW_TILE
    out_cols = out_weight.shape[1]
    bf16 = jnp.bfloat16
    chunk = (n, slots, width)
    half_chunk = (n // 2, slots, width)
    rows = (tokens, width)
    vmem = pl.BlockSpec(memory_space=pltpu.VMEM)
    hbm = pl.BlockSpec(memory_space=pl.ANY)
    return pl.pallas_call(
        functools.partial(fused_kernel, n, slots, reach),
        out_shape=(
            pltpu.VMEM((parts * tokens, out_cols), bf16),
            pltpu.VMEM(rows, bf16),
        ),
        in_specs=[hbm, hbm, vmem, hbm, hbm, vmem, hbm, hbm, hbm, hbm, hbm, hbm, vmem, vmem],
        out_specs=(vmem, vmem),
        scratch_shapes=[
            pltpu.VMEM(chunk, bf16),
            pltpu.VMEM(half_chunk, bf16),
            pltpu.VMEM((n, parts, slots, width), bf16),
            pltpu.VMEM((n, parts, slots, width), bf16),
            pltpu.VMEM((2,) + chunk, bf16),
            pltpu.VMEM(chunk, bf16),
            pltpu.VMEM(chunk, bf16),
            pltpu.VMEM(chunk, bf16),
            pltpu.VMEM(chunk, bf16),
            pltpu.VMEM(chunk, bf16),
            pltpu.VMEM(half_chunk, bf16),
            pltpu.VMEM(rows, bf16),
            pltpu.VMEM(rows, bf16),
            pltpu.VMEM((2, tokens), jnp.float32),
            pltpu.VMEM(rows, bf16),
            pltpu.VMEM(rows, bf16),
            pltpu.VMEM(rows, jnp.float32),
            pltpu.VMEM((halo_rows, width), bf16),
            pltpu.VMEM((halo_rows + tokens, width), jnp.float32),
            pltpu.VMEM(rows, jnp.float32),
            pltpu.VMEM((parts, tokens, width), bf16),
            pltpu.VMEM(rows, bf16),
            pltpu.VMEM((reach + 1, width), jnp.float32),
            pltpu.VMEM(rows, bf16),
            pltpu.VMEM((width, hidden), bf16),
            pltpu.VMEM((width, hidden), bf16),
            pltpu.VMEM((hidden, width), bf16),
            pltpu.VMEM((width, shared_hidden), bf16),
            pltpu.VMEM((width, shared_hidden), bf16),
            pltpu.VMEM((shared_hidden, width), bf16),
            pltpu.VMEM((width, out_cols), bf16),
            pltpu.SemaphoreType.DMA((10,)),
            pltpu.SemaphoreType.DMA((9, n)),
            pltpu.SemaphoreType.DMA((9, n)),
            pltpu.SemaphoreType.DMA((6 + CONV_PARTS,)),
            pltpu.SemaphoreType.DMA((6 + CONV_PARTS,)),
        ],
        compiler_params=pltpu.CompilerParams(
            collective_id=0, has_side_effects=True, vmem_limit_bytes=60 * 1024 * 1024
        ),
    )(
        conv_input,
        conv_kernel,
        conv_gain.reshape(1, width),
        out_weight,
        moe_input,
        moe_gain.reshape(1, width),
        expert_gate,
        expert_up,
        expert_down,
        shared_gate,
        shared_up,
        shared_down,
        expert_index.T,
        routing_weight.T,
    )


def fits_fused(args):
    n, parts = lax.axis_size("ep"), lax.axis_size("tp")
    conv_input, conv_kernel, moe_input = args[0], args[1], args[4]
    top_count = args[13].shape[1]
    tokens, width = moe_input.shape
    slots = 3 * tokens * top_count // (2 * n)
    return (
        parts == 4
        and top_count == 2
        and args[6].shape[0] == 1
        and conv_input.shape == moe_input.shape
        and conv_kernel.shape[0] - 1 <= tokens
        and tokens % LANES == 0
        and width % COLS == 0
        and slots % ROW_TILE == 0
        and slots >= ROW_TILE
        and n == 8
    )


def either(*args):
    return fused(*args) if fits_fused(args) else on_device(*args)


def solution(mesh):
    in_specs = (
        P(("ep", "tp"), None),
        P(),
        P(),
        P(None, "tp"),
        P(("ep", "tp"), None),
        P(),
        P("ep", None, "tp"),
        P("ep", None, "tp"),
        P("ep", "tp", None),
        P(),
        P(),
        P(),
        P("ep", None),
        P(("ep", "tp"), None),
    )
    out_specs = (P("ep", "tp"), P(("ep", "tp"), None))
    return jax.shard_map(
        either, mesh=mesh, in_specs=in_specs, out_specs=out_specs, check_vma=False
    )
```
